256 devices in a mesh: sp: 64 (over z, x, core), tp: 4 (over y).
Axes of the slice: x: 4, y: 4, z: 8, core: 2. Of those that a mesh axis runs over, the one named last changes fastest.
Arguments:
- residual: bfloat16 [65536, 2048], P('sp'), may hold values from -6 to 6
- query: bfloat16 [65536, 1024], P('sp', 'tp'), may hold values from -6 to 6
- key: bfloat16 [65536, 256], P('sp', 'tp'), may hold values from -6 to 6
- value: bfloat16 [65536, 256], P('sp', 'tp'), may hold values from -6 to 6
- sink: float32 [16], P('tp'), may hold values from 3 to 9
- norm_gain: float32 [2048], replicated, may hold values from 0.1 to 1.9
- w_out: bfloat16 [1024, 2048], P('tp'), may hold values from -1.5 to 1.5
- w_gate: bfloat16 [2048, 4096], P('sp', 'tp'), may hold values from -0.125 to 0.125
- w_value: bfloat16 [2048, 4096], P('sp', 'tp'), may hold values from -0.125 to 0.125
- conv_gate: bfloat16 [3, 4096], P(None, 'tp'), may hold values from -3 to 3
- conv_value: bfloat16 [3, 4096], P(None, 'tp'), may hold values from -3 to 3
- w_down: bfloat16 [4096, 2048], P('tp', 'sp'), may hold values from -0.09375 to 0.09375
Outputs:
- layer_out: bfloat16 [65536, 2048], P(('sp', 'tp'))
The draws below stay inside these ranges and needn't reach their ends.
All inputs are finite; a program needn't handle non-finite values.
Results may differ from the reference program's by a relative error of at most 0.015.
Values may be sent and summed in bfloat16 or wider, within the bound.
A program may use at most 128 MiB of HBM per device.

```python
import jax
import jax.numpy as jnp
from jax import lax

D = 2048
FF = 4096
HEADS = 16
KV_HEADS = 4
HD = 64
WINDOW = 128
TOKENS = 65536
N_TP = 4


def draw_key(key, part):
    base = jax.random.fold_in(key, 11)
    shape = (TOKENS, KV_HEADS * HD)
    return jnp.clip(jax.random.normal(jax.random.fold_in(base, 1), shape, jnp.float32), -6.0, 6.0).astype(jnp.bfloat16)


def draw_query(key, part):
    base = jax.random.fold_in(key, 11)
    shape = (TOKENS, HEADS * HD)
    return jnp.clip(jax.random.normal(jax.random.fold_in(base, 2), shape, jnp.float32), -6.0, 6.0).astype(jnp.bfloat16)


def steps_of(key, shape, split, smallest, top_value):
    level = 1.0
    for dim, shards_of in split:
        heights = jax.random.uniform(jax.random.fold_in(jax.random.fold_in(key, 6), dim), (shards_of,), jnp.float32, smallest / len(split), top_value / len(split))
        level = level * jnp.repeat(jnp.exp(heights), shape[dim] // shards_of).reshape((-1,) + (1,) * (len(shape) - 1 - dim))
    return level


def bell_draw(stream_key, dims, scale, most, shards=(), held_as=jnp.bfloat16):
    level = steps_of(stream_key, dims, shards, -0.22, 0.18) if shards else 1.0
    array = jax.random.normal(stream_key, dims, jnp.float32) * scale * level
    return jnp.minimum(jnp.maximum(array, -most), most).astype(held_as)


def setup_inputs(seed: int = 0) -> dict:
    key_of = jax.random.split(jax.random.key(seed), 13)
    residual = bell_draw(key_of[0], (TOKENS, D), 1.0, 6.0, ((0, 64),))
    query = draw_query(jax.random.fold_in(key_of[12], 71), 0)
    key = draw_key(jax.random.fold_in(key_of[12], 71), 0)
    value = bell_draw(key_of[3], (TOKENS, KV_HEADS * HD), 1.0, 6.0, ((0, 64), (1, 4)))
    sink = jnp.clip(3.0 + 6.0 * jax.random.uniform(key_of[4], (HEADS,), jnp.float32) ** steps_of(key_of[4], (HEADS,), ((0, 4),), -0.2, 0.2), 3.0, 9.0)
    norm_gain = jnp.clip(1.0 + 0.18 * jax.random.normal(key_of[5], (D,), jnp.float32), 0.1, 1.9)
    w_out = bell_draw(key_of[6], (HEADS * HD, D), (HD // 4) ** -0.5, 1.5, ((0, 4),))
    w_gate = bell_draw(key_of[7], (D, FF), D ** -0.5, 0.125, ((0, 64), (1, 4)))
    w_value = bell_draw(key_of[8], (D, FF), D ** -0.5, 0.125, ((0, 64), (1, 4)))
    conv_gate = bell_draw(key_of[9], (3, FF), 0.577, 3.0, ((1, 4),))
    conv_value = bell_draw(key_of[10], (3, FF), 0.577, 3.0, ((1, 4),))
    w_down = bell_draw(key_of[11], (FF, D), FF ** -0.5, 0.09375, ((0, 4), (1, 64)))
    return {"residual": residual, "query": query, "key": key, "value": value, "sink": sink, "norm_gain": norm_gain, "w_out": w_out, "w_gate": w_gate, "w_value": w_value, "conv_gate": conv_gate, "conv_value": conv_value, "w_down": w_down}


THETA = 10000.0
EPS = 1e-06

def rotate(field, positions):
    count = field.shape[0]
    parts = field.astype(jnp.float32).reshape(count, -1, HD)
    inverse = 1.0 / THETA ** (jnp.arange(0, HD, 2, dtype=jnp.float32) / HD)
    angle = positions[:, None] * inverse[None, :]
    cosine = jnp.cos(angle)[:, None, :]
    sine = jnp.sin(angle)[:, None, :]
    first = parts[..., :HD // 2]
    second = parts[..., HD // 2:]
    turned = jnp.concatenate([first * cosine - second * sine, second * cosine + first * sine], axis=-1)
    return turned.reshape(count, -1).astype(jnp.bfloat16)

def band_attention(queries, keys, values, sinks, start, total):
    count = queries.shape[0]
    blocks = count // WINDOW
    kv_local = keys.shape[1] // HD
    group = queries.shape[1] // (kv_local * HD)
    query_blocks = queries.astype(jnp.float32).reshape(blocks, WINDOW, kv_local, group, HD)
    key_band = jnp.concatenate([keys[i * WINDOW:i * WINDOW + count].reshape(blocks, WINDOW, kv_local, HD) for i in range(3)], axis=1).astype(jnp.float32)
    value_band = jnp.concatenate([values[i * WINDOW:i * WINDOW + count].reshape(blocks, WINDOW, kv_local, HD) for i in range(3)], axis=1).astype(jnp.float32)
    scores = jnp.einsum('nqkgd,njkd->nkgqj', query_blocks, key_band) * HD ** (-0.5)
    block_ids = jnp.arange(blocks, dtype=jnp.int32)[:, None]
    query_pos = start + block_ids * WINDOW + jnp.arange(WINDOW, dtype=jnp.int32)[None, :]
    key_pos = start - WINDOW + block_ids * WINDOW + jnp.arange(3 * WINDOW, dtype=jnp.int32)[None, :]
    valid = (key_pos[:, None, :] >= 0) & (key_pos[:, None, :] < total) & (jnp.abs(query_pos[:, :, None] - key_pos[:, None, :]) <= WINDOW)
    scores = jnp.where(valid[:, None, None], scores, -1e+30)
    sink_col = sinks.astype(jnp.float32).reshape(1, kv_local, group, 1, 1)
    top = jnp.maximum(lax.optimization_barrier(jnp.max(scores, axis=-1, keepdims=True)), sink_col)
    weights = jnp.exp(scores - top)
    denom = lax.optimization_barrier(jnp.sum(weights, axis=-1, keepdims=True)) + jnp.exp(sink_col - top)
    probs = (weights / denom).astype(jnp.bfloat16)
    out = jnp.einsum('nkgqj,njkd->nqkgd', probs.astype(jnp.float32), value_band)
    return out.reshape(count, kv_local * group * HD).astype(jnp.bfloat16)

def rmsnorm(field, gain):
    wide = field.astype(jnp.float32)
    scale = lax.rsqrt(lax.optimization_barrier(jnp.mean(wide * wide, axis=-1, keepdims=True)) + EPS)
    return (wide * scale * gain).astype(jnp.bfloat16)

def block_sum(left, right, pieces):
    width = left.shape[1] // pieces
    summed = jnp.zeros((left.shape[0], right.shape[1]), jnp.float32)
    for index in range(pieces):
        term = jnp.dot(left[:, index * width:(index + 1) * width], right[index * width:(index + 1) * width], preferred_element_type=jnp.float32)
        rounded = lax.optimization_barrier(term.astype(jnp.bfloat16))
        summed = summed + rounded.astype(jnp.float32)
    return summed

def reference(residual, query, key, value, sink, norm_gain, w_out, w_gate, w_value, conv_gate, conv_value, w_down):
    total = query.shape[0]
    kv_heads = key.shape[1] // HD
    group = query.shape[1] // key.shape[1]
    positions = jnp.arange(total, dtype=jnp.float32)
    turned_query = rotate(query, positions)
    turned_key = rotate(key, positions)
    pad = ((WINDOW, WINDOW), (0, 0))
    keys_ext = jnp.pad(turned_key, pad)
    values_ext = jnp.pad(value, pad)
    query_heads = turned_query.reshape(total, kv_heads, group * HD).transpose(1, 0, 2)
    key_heads = keys_ext.reshape(total + 2 * WINDOW, kv_heads, HD).transpose(1, 0, 2)
    value_heads = values_ext.reshape(total + 2 * WINDOW, kv_heads, HD).transpose(1, 0, 2)
    sink_heads = sink.reshape(kv_heads, group)

    def one_head(args):
        return band_attention(args[0], args[1], args[2], args[3], 0, total)
    outs = lax.map(one_head, (query_heads, key_heads, value_heads, sink_heads))
    attended = outs.transpose(1, 0, 2).reshape(total, -1)
    mix = block_sum(attended, w_out, N_TP)
    mid = (residual.astype(jnp.float32) + mix).astype(jnp.bfloat16)
    normed = rmsnorm(mid, norm_gain)
    gate_up = jnp.dot(normed, w_gate, preferred_element_type=jnp.float32).astype(jnp.bfloat16)
    value_up = jnp.dot(normed, w_value, preferred_element_type=jnp.float32).astype(jnp.bfloat16)

    def convolve(field, taps):
        padded = jnp.pad(field, ((1, 1), (0, 0))).astype(jnp.float32)
        taps = taps.astype(jnp.float32)
        return padded[:-2] * taps[0] + padded[1:-1] * taps[1] + padded[2:] * taps[2]
    gate_conv = convolve(gate_up, conv_gate)
    value_conv = convolve(value_up, conv_value)
    hidden = (jax.nn.silu(gate_conv) * value_conv).astype(jnp.bfloat16)
    ffn = block_sum(hidden, w_down, N_TP)
    return (mid.astype(jnp.float32) + ffn).astype(jnp.bfloat16)
```

```python
import functools

import jax
import jax.numpy as jnp
from jax import lax
from jax.experimental import pallas as pl
from jax.experimental.pallas import tpu as pltpu
from jax.sharding import PartitionSpec as P

HD = 64
WINDOW = 128
THETA = 10000.0
EPS = 1e-06
MESH = pl.DeviceIdType.MESH

NZ, NX, NC, NY = 8, 4, 2, 4
ROWS = 1024
D = 2048
FL = 1024
QC = 256
CH = 256
HALO = 16
NSEM = 112
NLOC = 8
NT = (((1,), (1,)), ((), ()))
F32 = jnp.float32
BF16 = jnp.bfloat16


class Comm:
    def __init__(self, send, recv, local):
        self.send, self.recv, self.local = send, recv, local
        self.count, self.lcount = 0, 0
        self.all = []

    def start(self, src, dst, **where):
        k = self.count
        self.count += 1
        copy = pltpu.make_async_remote_copy(
            src_ref=src,
            dst_ref=dst,
            send_sem=self.send.at[k],
            recv_sem=self.recv.at[k],
            device_id=where,
            device_id_type=MESH,
        )
        copy.start()
        self.all.append(copy)
        return copy

    def here(self, src, dst):
        copy = pltpu.make_async_copy(src, dst, self.local.at[self.lcount])
        self.lcount += 1
        copy.start()
        return copy


def turned(x, cosine, sine):
    lane = lax.broadcasted_iota(jnp.int32, x.shape, 1)
    other = jnp.where((lane & 63) < 32, pltpu.roll(x, 96, 1), pltpu.roll(x, 32, 1))
    return x * cosine + other * sine


def layer(
    sink_ref,
    q_ref,
    kv_ref,
    cos_ref,
    sin_ref,
    gain_ref,
    taps_ref,
    res_hbm,
    wo_hbm,
    g_hbm,
    vd_hbm,
    out_ref,
    kvx,
    qr,
    ka,
    kb,
    va,
    vb,
    att,
    wo,
    res,
    nrm,
    edge,
    g,
    vd,
    hid,
    part,
    own,
    rin,
    fin,
    send,
    recv,
    local,
):
    s = lax.axis_index("sp")
    t = lax.axis_index("tp")
    nsp = NZ * NX * NC
    z, x, c = s // (NX * NC), (s // NC) % NX, s % NC

    def at(dz, dx, dc=0):
        return (((z + dz + NZ) % NZ) * NX + (x + dx + NX) % NX) * NC + (c + dc) % NC

    def zi(dz):
        return (z + dz + NZ) % NZ

    def xi(dx):
        return (x + dx + NX) % NX

    ahead, behind = (s + 1) % nsp, (s + nsp - 1) % nsp
    mate = at(0, 0, 1)
    ty = [(t + k) % NY for k in range(NY)]

    barrier = pltpu.get_barrier_semaphore()
    peers = [{"sp": i} for i in (ahead, behind, at(1, 0), at(-1, 0), at(0, 1), at(0, 2), at(0, 3), mate)]
    peers += [{"tp": ty[k]} for k in (1, 2, 3)]
    for peer in peers:
        pl.semaphore_signal(barrier, inc=1, device_id=peer, device_id_type=MESH)
    pl.semaphore_wait(barrier, len(peers))

    cm = Comm(send, recv, local)

    h_low = cm.start(kv_ref.at[pl.ds(ROWS - WINDOW, WINDOW)], kvx.at[pl.ds(0, WINDOW)], sp=ahead)
    h_high = cm.start(kv_ref.at[pl.ds(0, WINDOW)], kvx.at[pl.ds(WINDOW + ROWS, WINDOW)], sp=behind)
    l_kv = cm.here(kv_ref, kvx.at[pl.ds(WINDOW, ROWS)])

    def vcell(dz, dx=0):
        return vd.at[zi(dz), xi(dx), c]

    def grow(dz):
        return g.at[zi(dz), :, c]

    vright = {0: cm.start(vd_hbm, vcell(0), sp=at(1, 0))}
    vleft = {0: cm.start(vd_hbm, vcell(0), sp=at(-1, 0))}
    g_x = [cm.start(g_hbm, g.at[z, x, c], sp=at(0, k)) for k in (1, 2, 3)]
    vx = {0: (cm.start(vd_hbm, vcell(0), sp=at(0, 1)), cm.start(vd_hbm, vcell(0), sp=at(0, -1)))}
    half = pl.ds(pl.multiple_of(c * 128, 128), 128)
    worow = pl.ds(pl.multiple_of(t * QC + c * 128, 128), 128)
    wo_y = [cm.start(wo_hbm.at[half], wo.at[worow], tp=ty[k]) for k in (1, 3, 2)]
    v_push = [cm.start(vd_hbm, vcell(0), sp=mate)]
    l_g = cm.here(g_hbm, g.at[z, x, c])
    l_v = cm.here(vd_hbm, vcell(0))
    l_wo = cm.here(wo_hbm, wo.at[pl.ds(pl.multiple_of(t * QC, QC), QC)])
    l_res = cm.here(res_hbm, res)

    @pl.loop(0, ROWS // WINDOW)
    def _(b):
        rows = pl.ds(pl.multiple_of(b * WINDOW, WINDOW), WINDOW)
        trows = pl.ds(pl.multiple_of(b * WINDOW + WINDOW, WINDOW), WINDOW)
        for p in range(2):
            lanes = slice(p * 128, p * 128 + 128)
            qr[rows, lanes] = turned(
                q_ref[rows, lanes].astype(F32), cos_ref[trows, :], sin_ref[trows, :]
            ).astype(BF16)

    l_kv.wait()
    h_low.wait_recv()
    h_high.wait_recv()

    @pl.loop(0, ROWS // WINDOW + 2)
    def _(b):
        rows = pl.ds(pl.multiple_of(b * WINDOW, WINDOW), WINDOW)
        both = kvx[rows, :].astype(F32)
        lane = lax.broadcasted_iota(jnp.int32, both.shape, 1)
        keys = jnp.where(lane < HD, turned(both, cos_ref[rows, :], sin_ref[rows, :]), 0.0)
        values = jnp.where(lane < HD, 0.0, both)
        ka[rows, :] = keys.astype(BF16)
        kb[rows, :] = pltpu.roll(keys, HD, 1).astype(BF16)
        va[rows, :] = pltpu.roll(values, HD, 1).astype(BF16)
        vb[rows, :] = values.astype(BF16)

    def attend(b):
        start = pl.multiple_of(b * WINDOW, WINDOW)
        rows = pl.ds(start, WINDOW)
        band = pl.ds(start, 3 * WINDOW)
        r = lax.broadcasted_iota(jnp.int32, (WINDOW, 3 * WINDOW), 0)
        j = lax.broadcasted_iota(jnp.int32, (WINDOW, 3 * WINDOW), 1)
        first = s * ROWS + start - WINDOW
        valid = (j >= r) & (j <= r + 2 * WINDOW) & (j + first >= 0) & (j + first < nsp * ROWS)
        lane = lax.broadcasted_iota(jnp.int32, (WINDOW, 128), 1)
        vv = jnp.concatenate([va[band, :], vb[band, :]], axis=0)
        for p in range(2):
            qp = qr[rows, p * 128 : p * 128 + 128]
            weights, inverse = [], []
            for i, keys in enumerate((ka, kb)):
                sc = lax.dot_general(qp, keys[band, :], NT, preferred_element_type=F32)
                sc = jnp.where(valid, sc * HD ** (-0.5), -1e30)
                sink = sink_ref[2 * p + i]
                top = jnp.maximum(jnp.max(sc, axis=1, keepdims=True), sink)
                w = jnp.exp(sc - top)
                denom = jnp.sum(w, axis=1, keepdims=True) + jnp.exp(sink - top)
                weights.append(w.astype(BF16))
                inverse.append(1.0 / denom)
            o = jnp.dot(jnp.concatenate(weights, axis=1), vv, preferred_element_type=F32)
            o = o * jnp.where(lane < HD, inverse[0], inverse[1])
            att[rows, pl.ds(pl.multiple_of(t * QC + p * 128, 128), 128)] = o.astype(BF16)

    def attend_chunk(ci):
        @pl.loop(0, 2)
        def _(i):
            attend(ci * 2 + i)

    a_y = {}

    def send_att(ci):
        piece = att.at[pl.ds(ci * CH, CH), pl.ds(pl.multiple_of(t * QC, QC), QC)]
        a_y[ci] = [cm.start(piece, piece, tp=ty[k]) for k in (1, 3, 2)]

    gright, gleft, g_push, vfwd, v_cols = {}, {}, [], {}, []

    def g_first():
        l_g.wait()
        for copy in g_x:
            copy.wait_recv()
        gright[0] = cm.start(grow(0), grow(0), sp=at(1, 0))
        gleft[0] = cm.start(grow(0), grow(0), sp=at(-1, 0))
        g_push.append(cm.start(grow(0), grow(0), sp=mate))

    def v_round(k):
        vright[k - 1].wait_recv()
        cell = vcell(-k)
        if k < 4:
            vright[k] = cm.start(cell, cell, sp=at(1, 0))
        vx[-k] = (cm.start(cell, cell, sp=at(0, 1)), cm.start(cell, cell, sp=at(0, -1)))
        v_push.append(cm.start(cell, cell, sp=mate))
        if k < 4:
            vleft[k - 1].wait_recv()
            cell = vcell(k)
            if k < 3:
                vleft[k] = cm.start(cell, cell, sp=at(-1, 0))
            vx[k] = (cm.start(cell, cell, sp=at(0, 1)), cm.start(cell, cell, sp=at(0, -1)))
            v_push.append(cm.start(cell, cell, sp=mate))

    def v_across(o):
        vx[o][0].wait_recv()
        vx[o][1].wait_recv()
        if o >= 0:
            vfwd[o] = cm.start(vcell(o, -1), vcell(o, -1), sp=at(0, 1))
        else:
            vfwd[o] = cm.start(vcell(o, 1), vcell(o, 1), sp=at(0, -1))

    def g_round(k):
        gright[k - 1].wait_recv()
        if k < 4:
            gright[k] = cm.start(grow(-k), grow(-k), sp=at(1, 0))
        g_push.append(cm.start(grow(-k), grow(-k), sp=mate))
        if k < 4:
            gleft[k - 1].wait_recv()
            if k < 3:
                gleft[k] = cm.start(grow(k), grow(k), sp=at(-1, 0))
            g_push.append(cm.start(grow(k), grow(k), sp=mate))

    scale_of = 1.0 / D
    wo_push = []

    def wo_arrived():
        l_wo.wait()
        for i, k in enumerate((1, 3, 2)):
            wo_y[i].wait_recv()
            rows = pl.ds(pl.multiple_of(((t + NY - k) % NY) * QC + c * 128, 128), 128)
            wo_push.append(cm.start(wo.at[rows], wo.at[rows], sp=mate))

    def middle(ci):
        for copy in a_y[ci]:
            copy.wait_recv()
        rows = pl.ds(ci * CH, CH)
        nrows = pl.ds(HALO + ci * CH, CH)

        def column(n, total):
            cols = pl.ds(pl.multiple_of(n * 256, 256), 256)
            mid = res[rows, cols].astype(F32) + jnp.dot(att[rows, :], wo[:, cols], preferred_element_type=F32)
            mid = mid.astype(BF16)
            res[rows, cols] = mid
            wide = mid.astype(F32)
            return total + jnp.sum(wide * wide, axis=1, keepdims=True)

        total = lax.fori_loop(0, D // 256, column, jnp.zeros((CH, 1), F32))
        scale = lax.rsqrt(total * scale_of + EPS)

        @pl.loop(0, D // 256)
        def _(n):
            cols = pl.ds(pl.multiple_of(n * 256, 256), 256)
            nrm[nrows, cols] = (res[rows, cols].astype(F32) * scale * gain_ref[:, cols]).astype(BF16)

    def up(tc):
        rows = pl.ds(pl.multiple_of(tc * CH, CH), CH + 2 * HALO)

        @pl.loop(0, FL // 256)
        def _(n):
            cols = pl.ds(pl.multiple_of(n * 256, 256), 256)
            field = nrm[rows, :]

            def convolved(weight, tap):
                u = jnp.dot(field, weight.reshape(D, 256), preferred_element_type=F32)
                u = u.astype(BF16).astype(F32)
                return (
                    u[HALO - 1 : HALO - 1 + CH] * taps_ref[tap : tap + 1, cols]
                    + u[HALO : HALO + CH] * taps_ref[tap + 1 : tap + 2, cols]
                    + u[HALO + 1 : HALO + 1 + CH] * taps_ref[tap + 2 : tap + 3, cols]
                )

            gate = convolved(g[:, :, :, :, cols], 0)
            value = convolved(vd[:, :, :, 0, :, cols], 3)
            hid[:, cols] = (gate / (1.0 + jnp.exp(-gate)) * value).astype(BF16)

    def down(into):
        @pl.loop(0, D // 256)
        def _(n):
            cols = pl.ds(pl.multiple_of(n * 256, 256), 256)
            term = lax.dot_general(hid[...], vd[n, :, :, 1].reshape(256, FL), NT, preferred_element_type=F32)
            into[:, cols] = term.astype(into.dtype)

    attend_chunk(0)
    g_first()
    v_round(1)
    attend_chunk(3)
    send_att(0)
    v_across(0)
    attend_chunk(1)
    send_att(3)
    v_round(2)
    g_round(1)
    attend_chunk(2)
    send_att(1)
    v_across(1)
    v_across(-1)
    l_v.wait()
    v_round(3)
    send_att(2)
    g_round(2)
    v_across(2)
    v_across(-2)
    wo_arrived()
    v_round(4)
    g_round(3)
    v_across(3)
    v_across(-3)
    l_res.wait()
    for copy in wo_push:
        copy.wait_recv()
    middle(0)
    v_across(-4)
    g_round(4)
    middle(3)
    e_high = cm.start(nrm.at[pl.ds(HALO, HALO)], edge.at[1], sp=behind)
    for o in vfwd:
        vfwd[o].wait_recv()
    for k in (1, 2, 3):
        column = vd.at[:, xi(k), c]
        v_cols.append(cm.start(column, column, sp=mate))
    middle(1)
    e_low = cm.start(nrm.at[pl.ds(ROWS, HALO)], edge.at[0], sp=ahead)
    middle(2)
    e_high.wait_recv()
    e_low.wait_recv()
    nrm[0:HALO, :] = jnp.where(s > 0, edge[0].astype(F32), 0.0).astype(BF16)
    nrm[HALO + ROWS :, :] = jnp.where(s < nsp - 1, edge[1].astype(F32), 0.0).astype(BF16)
    for copy in g_push + v_push + v_cols:
        copy.wait_recv()

    up(ty[2])
    down(part.at[0])
    s_right = cm.start(part.at[0, pl.ds(0, 128)], rin.at[0], tp=ty[1])
    s_left = cm.start(part.at[0, pl.ds(128, 128)], rin.at[1], tp=ty[3])
    up(ty[1])
    down(part.at[1])
    b_right = cm.start(part.at[1, pl.ds(128, 128)], fin.at[1], tp=ty[1])
    up(ty[3])
    down(part.at[2])
    a_left = cm.start(part.at[2, pl.ds(0, 128)], fin.at[2], tp=ty[3])
    s_right.wait_recv()

    @pl.loop(0, 8)
    def _(n):
        cols = pl.ds(pl.multiple_of(n * 256, 256), 256)
        part[1, 0:128, cols] = (part[1, 0:128, cols].astype(F32) + rin[0, :, cols].astype(F32)).astype(BF16)

    a_right = cm.start(part.at[1, pl.ds(0, 128)], fin.at[0], tp=ty[1])
    s_left.wait_recv()

    @pl.loop(0, 8)
    def _(n):
        cols = pl.ds(pl.multiple_of(n * 256, 256), 256)
        part[2, 128:256, cols] = (part[2, 128:256, cols].astype(F32) + rin[1, :, cols].astype(F32)).astype(BF16)

    b_left = cm.start(part.at[2, pl.ds(128, 128)], fin.at[3], tp=ty[3])
    up(t)
    down(own)
    for copy in (b_right, a_left, a_right, b_left):
        copy.wait_recv()

    @pl.loop(0, 8)
    def _(n):
        cols = pl.ds(pl.multiple_of(n * 256, 256), 256)
        for i in range(2):
            rows = slice(i * 128, i * 128 + 128)
            mrows = pl.ds(pl.multiple_of(t * CH + i * 128, 128), 128)
            ffn = own[rows, cols] + fin[i, :, cols].astype(F32) + fin[2 + i, :, cols].astype(F32)
            out_ref[rows, cols] = (res[mrows, cols].astype(F32) + ffn).astype(BF16)

    for copy in cm.all:
        copy.wait_send()


def shards(
    residual,
    query,
    key,
    value,
    sink,
    norm_gain,
    w_out,
    w_gate,
    w_value,
    conv_gate,
    conv_value,
    w_down,
):
    offset = lax.axis_index("sp") * ROWS
    positions = (offset - WINDOW + jnp.arange(ROWS + 2 * WINDOW, dtype=jnp.int32)).astype(F32)
    inverse = 1.0 / THETA ** (jnp.arange(0, HD, 2, dtype=F32) / HD)
    angle = positions[:, None] * jnp.tile(inverse, 4)[None, :]
    sign = jnp.where(jnp.arange(128) % HD < HD // 2, -1.0, 1.0).astype(F32)
    cosine = jnp.cos(angle)
    sine = jnp.sin(angle) * sign[None, :]
    kv = jnp.concatenate([key, value], axis=1)
    vd_own = jnp.stack([w_value, w_down.T])
    taps = jnp.concatenate([conv_gate, conv_value], axis=0).astype(F32)
    vmem = pl.BlockSpec(memory_space=pltpu.VMEM)
    hbm = pl.BlockSpec(memory_space=pl.ANY)
    return pl.pallas_call(
        layer,
        out_shape=jax.ShapeDtypeStruct((CH, D), BF16),
        in_specs=[pl.BlockSpec(memory_space=pltpu.SMEM)] + [vmem] * 6 + [hbm] * 4,
        out_specs=vmem,
        scratch_shapes=[
            pltpu.VMEM((ROWS + 2 * WINDOW, 128), BF16),
            pltpu.VMEM((ROWS, QC), BF16),
            pltpu.VMEM((ROWS + 2 * WINDOW, 128), BF16),
            pltpu.VMEM((ROWS + 2 * WINDOW, 128), BF16),
            pltpu.VMEM((ROWS + 2 * WINDOW, 128), BF16),
            pltpu.VMEM((ROWS + 2 * WINDOW, 128), BF16),
            pltpu.VMEM((ROWS, NY * QC), BF16),
            pltpu.VMEM((NY * QC, D), BF16),
            pltpu.VMEM((ROWS, D), BF16),
            pltpu.VMEM((ROWS + 2 * HALO, D), BF16),
            pltpu.VMEM((2, HALO, D), BF16),
            pltpu.VMEM((NZ, NX, NC, 32, FL), BF16),
            pltpu.VMEM((NZ, NX, NC, 2, 32, FL), BF16),
            pltpu.VMEM((CH, FL), BF16),
            pltpu.VMEM((3, CH, D), BF16),
            pltpu.VMEM((CH, D), F32),
            pltpu.VMEM((2, 128, D), BF16),
            pltpu.VMEM((4, 128, D), BF16),
            pltpu.SemaphoreType.DMA((NSEM,)),
            pltpu.SemaphoreType.DMA((NSEM,)),
            pltpu.SemaphoreType.DMA((NLOC,)),
        ],
        compiler_params=pltpu.CompilerParams(
            collective_id=0, has_side_effects=True, vmem_limit_bytes=60 * 1024 * 1024
        ),
        name="layer",
    )(sink, query, kv, cosine, sine, norm_gain.reshape(1, D), taps, residual, w_out, w_gate, vd_own)


def solution(mesh):
    return jax.shard_map(
        shards,
        mesh=mesh,
        in_specs=(
            P("sp", None),
            P("sp", "tp"),
            P("sp", "tp"),
            P("sp", "tp"),
            P("tp"),
            P(),
            P("tp", None),
            P("sp", "tp"),
            P("sp", "tp"),
            P(None, "tp"),
            P(None, "tp"),
            P("tp", "sp"),
        ),
        out_specs=P(("sp", "tp"), None),
        check_vma=False,
    )
```

```python
import functools

import jax
import jax.numpy as jnp
from jax import lax
from jax.experimental import pallas as pl
from jax.experimental.pallas import tpu as pltpu
from jax.sharding import PartitionSpec as P

HD = 64
WINDOW = 128
THETA = 10000.0
EPS = 1e-06
MESH = pl.DeviceIdType.MESH

NZ, NX, NC, NY = 8, 4, 2, 4
ROWS = 1024
D = 2048
FL = 1024
QC = 256
CH = 256
HALO = 16
NSEM = 184
NLOC = 12
NT = (((1,), (1,)), ((), ()))
F32 = jnp.float32
BF16 = jnp.bfloat16


class Comm:
    def __init__(self, send, recv, local):
        self.send, self.recv, self.local = send, recv, local
        self.count, self.lcount = 0, 0
        self.all = []

    def start(self, src, dst, **where):
        k = self.count
        self.count += 1
        copy = pltpu.make_async_remote_copy(
            src_ref=src,
            dst_ref=dst,
            send_sem=self.send.at[k],
            recv_sem=self.recv.at[k],
            device_id=where,
            device_id_type=MESH,
        )
        copy.start()
        self.all.append(copy)
        return copy

    def here(self, src, dst):
        copy = pltpu.make_async_copy(src, dst, self.local.at[self.lcount])
        self.lcount += 1
        copy.start()
        return copy


def turned(x, cosine, sine):
    lane = lax.broadcasted_iota(jnp.int32, x.shape, 1)
    other = jnp.where((lane & 63) < 32, pltpu.roll(x, 96, 1), pltpu.roll(x, 32, 1))
    return x * cosine + other * sine


def layer(
    sink_ref,
    cos_ref,
    sin_ref,
    q_hbm,
    gain_hbm,
    tap_gate_hbm,
    tap_value_hbm,
    key_hbm,
    value_hbm,
    res_hbm,
    wo_hbm,
    g_hbm,
    v_hbm,
    d_hbm,
    out_ref,
    q_ref,
    gain_ref,
    tap_gate,
    tap_value,
    kvx,
    qr,
    ka,
    kb,
    va,
    vb,
    att,
    wo,
    res,
    nrm,
    edge,
    g,
    v,
    d,
    wdown,
    hid,
    part,
    own,
    rin,
    fin,
    send,
    recv,
    local,
):
    s = lax.axis_index("sp")
    t = lax.axis_index("tp")
    nsp = NZ * NX * NC
    z, x, c = s // (NX * NC), (s // NC) % NX, s % NC

    def at(dz, dx, dc=0):
        return (((z + dz + NZ) % NZ) * NX + (x + dx + NX) % NX) * NC + (c + dc) % NC

    def zi(dz):
        return (z + dz + NZ) % NZ

    def xi(dx):
        return (x + dx + NX) % NX

    ahead, behind = (s + 1) % nsp, (s + nsp - 1) % nsp
    mate = at(0, 0, 1)
    ty = [(t + k) % NY for k in range(NY)]

    cm = Comm(send, recv, local)

    def cell(weight, dz, dx=0):
        return weight.at[zi(dz), xi(dx), c]

    def grow(dz):
        return g.at[zi(dz), :, c]

    l_v, l_d = cm.here(v_hbm, v.at[z, x, c]), cm.here(d_hbm, d.at[z, x, c])
    l_kv = [
        cm.here(key_hbm, kvx.at[0:HD, pl.ds(WINDOW, ROWS)]),
        cm.here(value_hbm, kvx.at[HD : 2 * HD, pl.ds(WINDOW, ROWS)]),
    ]
    l_wo = cm.here(wo_hbm, wo.at[pl.ds(pl.multiple_of(t * QC, QC), QC)])
    l_g = cm.here(g_hbm, g.at[z, x, c])
    l_q = cm.here(q_hbm, q_ref)
    l_small = [cm.here(gain_hbm, gain_ref), cm.here(tap_gate_hbm, tap_gate), cm.here(tap_value_hbm, tap_value)]
    l_res = cm.here(res_hbm, res)

    barrier = pltpu.get_barrier_semaphore()
    peers = [{"sp": i} for i in (ahead, behind, at(1, 0), at(-1, 0), at(0, 1), at(0, 2), at(0, 3), mate)]
    peers += [{"tp": ty[k]} for k in (1, 3)]
    for peer in peers:
        pl.semaphore_signal(barrier, inc=1, device_id=peer, device_id_type=MESH)
    pl.semaphore_wait(barrier, len(peers))

    l_v.wait()

    class Flow:
        def __init__(self, weight):
            self.weight = weight
            self.right, self.left, self.across, self.on = {}, {}, {}, {}
            self.push = []

        def begin(self):
            own = cell(self.weight, 0)
            self.right[0] = cm.start(own, own, sp=at(1, 0))
            self.left[0] = cm.start(own, own, sp=at(-1, 0))

        def share(self, o):
            self.push.append(cm.start(cell(self.weight, o), cell(self.weight, o), sp=mate))

        def spread(self, o):
            one = cell(self.weight, o)
            self.across[o] = (cm.start(one, one, sp=at(0, 1)), cm.start(one, one, sp=at(0, -1)))

        def round(self, k):
            self.right[k - 1].wait_recv()
            if k < 4:
                one = cell(self.weight, -k) if k < 3 else self.weight.at[zi(-k), x, c, pl.ds(0, 16)]
                self.right[k] = cm.start(one, one, sp=at(1, 0))
            self.left[k - 1].wait_recv()
            if k < 4:
                one = cell(self.weight, k) if k < 3 else self.weight.at[zi(k), x, c, pl.ds(16, 16)]
                self.left[k] = cm.start(one, one, sp=at(-1, 0))

        def pass_on(self, o):
            left, right = cell(self.weight, o, -1), cell(self.weight, o, 1)
            self.across[o][0].wait_recv()
            if o >= 0:
                self.on[o] = cm.start(left, left, sp=at(0, 1))
            self.push.append(cm.start(left, left, sp=mate))
            self.across[o][1].wait_recv()
            if o < 0:
                self.on[o] = cm.start(right, right, sp=at(0, -1))
            self.push.append(cm.start(right, right, sp=mate))

        def last(self, o):
            self.on[o].wait_recv()
            self.push.append(cm.start(cell(self.weight, o, 2), cell(self.weight, o, 2), sp=mate))

        def arrived(self):
            for copy in self.push:
                copy.wait_recv()

    fv, fd = Flow(v), Flow(d)
    fv.begin()
    fv.spread(0)
    for copy in l_kv:
        copy.wait()
    h_low = cm.start(kvx.at[:, pl.ds(ROWS, WINDOW)], kvx.at[:, pl.ds(0, WINDOW)], sp=ahead)
    h_high = cm.start(kvx.at[:, pl.ds(WINDOW, WINDOW)], kvx.at[:, pl.ds(WINDOW + ROWS, WINDOW)], sp=behind)
    l_wo.wait()

    def worows(k, at_row=0, count=128):
        return wo.at[pl.ds(pl.multiple_of(((t + k) % NY) * QC + c * 128 + at_row, 64), count)]

    wo_right = cm.start(worows(0), worows(0), tp=ty[1])
    wo_left = cm.start(worows(0), worows(0), tp=ty[3])
    l_g.wait()
    g_x = [cm.start(g.at[z, x, c], g.at[z, x, c], sp=at(0, k)) for k in (1, 3, 2)]
    fv.share(0)
    l_d.wait()
    fd.spread(0)

    def table(b):
        base = pl.ds(WINDOW + b, 1)
        cb, sb = cos_ref[base, :], sin_ref[base, :]
        cr, sr = cos_ref[0:WINDOW, :], sin_ref[0:WINDOW, :]
        lane = lax.broadcasted_iota(jnp.int32, (WINDOW, 128), 1)
        sine = sb * cr + cb * sr
        return cb * cr - sb * sr, jnp.where((lane & 63) < 32, -sine, sine)

    def prepare(b, with_query):
        cosine, sine = table(b)
        rows = pl.ds(pl.multiple_of(b * WINDOW, WINDOW), WINDOW)
        if with_query:
            qrows = pl.ds(pl.multiple_of(b * WINDOW - WINDOW, WINDOW), WINDOW)
            for p in range(2):
                lanes = slice(p * 128, p * 128 + 128)
                qr[qrows, lanes] = turned(q_ref[qrows, lanes].astype(F32), cosine, sine).astype(BF16)
        both = kvx[:, rows].astype(F32).T
        lane = lax.broadcasted_iota(jnp.int32, both.shape, 1)
        keys = jnp.where(lane < HD, turned(both, cosine, sine), 0.0)
        values = jnp.where(lane < HD, 0.0, both)
        ka[rows, :] = keys.astype(BF16)
        kb[rows, :] = pltpu.roll(keys, HD, 1).astype(BF16)
        va[rows, :] = pltpu.roll(values, HD, 1).astype(BF16)
        vb[rows, :] = values.astype(BF16)

    l_q.wait()

    @pl.loop(1, ROWS // WINDOW + 1)
    def _(b):
        prepare(b, True)

    h_low.wait_recv()
    h_high.wait_recv()

    @pl.loop(0, 2)
    def _(i):
        prepare(i * (ROWS // WINDOW + 1), False)

    def attend(b):
        start = pl.multiple_of(b * WINDOW, WINDOW)
        rows = pl.ds(start, WINDOW)
        band = pl.ds(start, 3 * WINDOW)
        r = lax.broadcasted_iota(jnp.int32, (WINDOW, 3 * WINDOW), 0)
        j = lax.broadcasted_iota(jnp.int32, (WINDOW, 3 * WINDOW), 1)
        first = s * ROWS + start - WINDOW
        valid = (j >= r) & (j <= r + 2 * WINDOW) & (j + first >= 0) & (j + first < nsp * ROWS)
        lane = lax.broadcasted_iota(jnp.int32, (WINDOW, 128), 1)
        vv = jnp.concatenate([va[band, :], vb[band, :]], axis=0)
        for p in range(2):
            qp = qr[rows, p * 128 : p * 128 + 128]
            weights, inverse = [], []
            for i, keys in enumerate((ka, kb)):
                sc = lax.dot_general(qp, keys[band, :], NT, preferred_element_type=F32)
                sc = jnp.where(valid, sc * HD ** (-0.5), -1e30)
                sink = sink_ref[2 * p + i]
                top = jnp.maximum(jnp.max(sc, axis=1, keepdims=True), sink)
                w = jnp.exp(sc - top)
                denom = jnp.sum(w, axis=1, keepdims=True) + jnp.exp(sink - top)
                weights.append(w.astype(BF16))
                inverse.append(1.0 / denom)
            o = jnp.dot(jnp.concatenate(weights, axis=1), vv, preferred_element_type=F32)
            o = o * jnp.where(lane < HD, inverse[0], inverse[1])
            att[rows, pl.ds(pl.multiple_of(t * QC + p * 128, 128), 128)] = o.astype(BF16)

    def attend_chunk(ci):
        @pl.loop(0, 2)
        def _(i):
            attend(ci * 2 + i)

    a_y, a_on = {}, {}

    def send_att(ci):
        piece = att.at[pl.ds(ci * CH, CH), pl.ds(pl.multiple_of(t * QC, QC), QC)]
        a_y[ci] = (cm.start(piece, piece, tp=ty[1]), cm.start(piece, piece, tp=ty[3]))

    def pass_att(ci):
        a_y[ci][0].wait_recv()
        piece = att.at[pl.ds(ci * CH, 128), pl.ds(pl.multiple_of(ty[3] * QC, QC), QC)]
        right = cm.start(piece, piece, tp=ty[1])
        a_y[ci][1].wait_recv()
        piece = att.at[pl.ds(ci * CH + 128, 128), pl.ds(pl.multiple_of(ty[1] * QC, QC), QC)]
        a_on[ci] = (right, cm.start(piece, piece, tp=ty[3]))

    wo_on, wo_push = [], []

    def pass_wo():
        wo_right.wait_recv()
        wo_on.append(cm.start(worows(3, 0, 64), worows(3, 0, 64), tp=ty[1]))
        wo_push.append(cm.start(worows(3), worows(3), sp=mate))
        wo_left.wait_recv()
        wo_on.append(cm.start(worows(1, 64, 64), worows(1, 64, 64), tp=ty[3]))
        wo_push.append(cm.start(worows(1), worows(1), sp=mate))

    def last_wo():
        for copy in wo_on:
            copy.wait_recv()
        wo_push.append(cm.start(worows(2), worows(2), sp=mate))

    gright, gleft, g_push = {}, {}, []

    def g_first():
        for copy in g_x:
            copy.wait_recv()
        gright[0] = cm.start(grow(0), grow(0), sp=at(1, 0))
        gleft[0] = cm.start(grow(0), grow(0), sp=at(-1, 0))
        g_push.append(cm.start(grow(0), grow(0), sp=mate))

    def g_round(k):
        gright[k - 1].wait_recv()
        if k < 4:
            block = grow(-k) if k < 3 else g.at[zi(-k), pl.ds(0, 2), c]
            gright[k] = cm.start(block, block, sp=at(1, 0))
        gleft[k - 1].wait_recv()
        if k < 4:
            block = grow(k) if k < 3 else g.at[zi(k), pl.ds(2, 2), c]
            gleft[k] = cm.start(block, block, sp=at(-1, 0))
            g_push.append(cm.start(grow(k), grow(k), sp=mate))
        g_push.append(cm.start(grow(-k), grow(-k), sp=mate))

    def middle(ci):
        for copy in a_on[ci]:
            copy.wait_recv()
        rows = pl.ds(ci * CH, CH)
        nrows = pl.ds(HALO + ci * CH, CH)
        total = jnp.zeros((CH, 1), F32)
        for n in range(D // 512):
            cols = slice(n * 512, n * 512 + 512)
            mid = res[rows, cols].astype(F32) + jnp.dot(att[rows, :], wo[:, cols], preferred_element_type=F32)
            mid = mid.astype(BF16)
            res[rows, cols] = mid
            wide = mid.astype(F32)
            total = total + jnp.sum(wide * wide, axis=1, keepdims=True)
        scale = lax.rsqrt(total / D + EPS)
        for n in range(D // 512):
            cols = slice(n * 512, n * 512 + 512)
            nrm[nrows, cols] = (res[rows, cols].astype(F32) * scale * gain_ref[:, cols]).astype(BF16)

    def up(tc):
        rows = pl.ds(pl.multiple_of(tc * CH, CH), CH + 2 * HALO)
        for n in range(FL // 512):
            cols = slice(n * 512, n * 512 + 512)

            def convolved(weight, taps_ref):
                u = jnp.dot(nrm[rows, :], weight.reshape(D, 512), preferred_element_type=F32)
                u = u.astype(BF16).astype(F32)
                taps = taps_ref[:, cols].astype(F32)
                return (
                    u[HALO - 1 : HALO - 1 + CH] * taps[0:1]
                    + u[HALO : HALO + CH] * taps[1:2]
                    + u[HALO + 1 : HALO + 1 + CH] * taps[2:3]
                )

            gate = convolved(g[:, :, :, :, cols], tap_gate)
            value = convolved(v[:, :, :, :, cols], tap_value)
            hid[:, cols] = (gate / (1.0 + jnp.exp(-gate)) * value).astype(BF16)

    def turn_down():
        for n in range(NZ):
            wdown[:, n * 256 : n * 256 + 256] = d[n].reshape(256, FL).T

    def down(into, tiles=range(D // 512)):
        for n in tiles:
            cols = slice(n * 512, n * 512 + 512)
            into[:, cols] = jnp.dot(hid[...], wdown[:, cols], preferred_element_type=F32).astype(into.dtype)

    attend_chunk(0)
    fv.round(1)
    for o in (1, -1):
        fv.spread(o)
        fv.share(o)
    fv.pass_on(0)
    fd.begin()
    attend_chunk(3)
    send_att(0)
    fv.round(2)
    g_first()
    for o in (2, -2):
        fv.spread(o)
        fv.share(o)
    attend_chunk(1)
    send_att(3)
    fd.round(1)
    fd.spread(1)
    fd.spread(-1)
    attend_chunk(2)
    fv.pass_on(1)
    fv.pass_on(-1)
    fd.pass_on(0)
    fv.last(0)
    fv.round(3)
    for o in (3, -3):
        fv.spread(o)
        fv.share(o)
    pass_wo()
    send_att(1)
    send_att(2)
    fd.round(2)
    g_round(1)
    fv.round(4)
    fv.spread(-4)
    fv.share(-4)
    fd.spread(2)
    fd.spread(-2)
    fv.pass_on(2)
    fv.pass_on(-2)
    fv.last(1)
    fv.last(-1)
    fd.share(0)
    pass_att(0)
    pass_att(3)
    fd.pass_on(1)
    fd.pass_on(-1)
    fd.round(3)
    fd.spread(3)
    fd.spread(-3)
    last_wo()
    fv.pass_on(3)
    fv.pass_on(-3)
    fv.pass_on(-4)
    pass_att(1)
    g_round(2)
    fd.round(4)
    fd.spread(-4)
    pass_att(2)
    for copy in [l_res] + l_small:
        copy.wait()
    fv.last(2)
    fv.last(-2)
    for o in (1, -1, 2, -2):
        fd.share(o)
    for copy in wo_push:
        copy.wait_recv()
    middle(0)
    fd.pass_on(2)
    fd.pass_on(-2)
    middle(3)
    g_round(3)
    e_high = cm.start(nrm.at[pl.ds(HALO, HALO)], edge.at[1], sp=behind)
    fd.pass_on(3)
    fd.pass_on(-3)
    fd.pass_on(-4)
    middle(1)
    e_low = cm.start(nrm.at[pl.ds(ROWS, HALO)], edge.at[0], sp=ahead)
    for o in (3, -3, -4):
        fv.last(o)
    for o in (0, 1, -1, 2, -2):
        fd.last(o)
    middle(2)
    g_round(4)
    for o in (3, -3, -4):
        fd.share(o)
        fd.last(o)
    fv.arrived()
    for copy in g_push:
        copy.wait_recv()
    e_high.wait_recv()
    e_low.wait_recv()
    nrm[0:HALO, :] = jnp.where(s > 0, edge[0].astype(F32), 0.0).astype(BF16)
    nrm[HALO + ROWS :, :] = jnp.where(s < nsp - 1, edge[1].astype(F32), 0.0).astype(BF16)
    fd.arrived()
    turn_down()
    up(ty[2])
    sides = (slice(0, D // 2), slice(D // 2, D))
    s_right, s_left = [], []
    for i, side in enumerate(sides):
        down(part.at[0], (2 * i, 2 * i + 1))
        s_right.append(cm.start(part.at[0, 0:128, side], rin.at[0, :, side], tp=ty[1]))
        s_left.append(cm.start(part.at[0, 128:256, side], rin.at[1, :, side], tp=ty[3]))
    up(ty[1])
    down(part.at[1])
    b_right = cm.start(part.at[1, 128:256], fin.at[1], tp=ty[1])
    up(ty[3])
    down(part.at[2])
    a_left = cm.start(part.at[2, 0:128], fin.at[2], tp=ty[3])

    def joined(which, rows, side):
        base = 0 if side.start == 0 else D // 2

        @pl.loop(0, 4)
        def _(n):
            cols = pl.ds(pl.multiple_of(base + n * 256, 256), 256)
            total = part[1 + which, rows, cols].astype(F32) + rin[which, :, cols].astype(F32)
            part[1 + which, rows, cols] = total.astype(BF16)

    a_right, b_left = [], []
    for i, side in enumerate(sides):
        s_right[i].wait_recv()
        joined(0, slice(0, 128), side)
        a_right.append(cm.start(part.at[1, 0:128, side], fin.at[0, :, side], tp=ty[1]))
        s_left[i].wait_recv()
        joined(1, slice(128, 256), side)
        b_left.append(cm.start(part.at[2, 128:256, side], fin.at[3, :, side], tp=ty[3]))
    up(t)
    down(own)
    b_right.wait_recv()
    a_left.wait_recv()
    for i, side in enumerate(sides):
        a_right[i].wait_recv()
        b_left[i].wait_recv()

        @pl.loop(4 * i, 4 * i + 4)
        def _(n):
            cols = pl.ds(pl.multiple_of(n * 256, 256), 256)
            for k in range(2):
                rows = slice(k * 128, k * 128 + 128)
                mrows = pl.ds(pl.multiple_of(t * CH + k * 128, 128), 128)
                ffn = own[rows, cols] + fin[k, :, cols].astype(F32) + fin[2 + k, :, cols].astype(F32)
                out_ref[rows, cols] = (res[mrows, cols].astype(F32) + ffn).astype(BF16)

    for copy in cm.all:
        copy.wait_send()


def shards(
    residual,
    query,
    key,
    value,
    sink,
    norm_gain,
    w_out,
    w_gate,
    w_value,
    conv_gate,
    conv_value,
    w_down,
):
    offset = lax.axis_index("sp") * ROWS
    inverse = 1.0 / THETA ** (jnp.arange(0, HD, 2, dtype=F32) / HD)
    within = jnp.arange(WINDOW, dtype=jnp.int32)
    starts = offset + (jnp.arange(16, dtype=jnp.int32) - 1) * WINDOW
    positions = jnp.concatenate([within, starts]).astype(F32)
    angle = positions[:, None] * jnp.tile(inverse, 4)[None, :]
    vmem = pl.BlockSpec(memory_space=pltpu.VMEM)
    hbm = pl.BlockSpec(memory_space=pl.ANY)
    return pl.pallas_call(
        layer,
        out_shape=jax.ShapeDtypeStruct((CH, D), BF16),
        in_specs=[pl.BlockSpec(memory_space=pltpu.SMEM)] + [vmem] * 2 + [hbm] * 11,
        out_specs=vmem,
        scratch_shapes=[
            pltpu.VMEM((ROWS, QC), BF16),
            pltpu.VMEM((1, D), F32),
            pltpu.VMEM((3, FL), BF16),
            pltpu.VMEM((3, FL), BF16),
            pltpu.VMEM((2 * HD, ROWS + 2 * WINDOW), BF16),
            pltpu.VMEM((ROWS, QC), BF16),
            pltpu.VMEM((ROWS + 2 * WINDOW, 128), BF16),
            pltpu.VMEM((ROWS + 2 * WINDOW, 128), BF16),
            pltpu.VMEM((ROWS + 2 * WINDOW, 128), BF16),
            pltpu.VMEM((ROWS + 2 * WINDOW, 128), BF16),
            pltpu.VMEM((ROWS, NY * QC), BF16),
            pltpu.VMEM((NY * QC, D), BF16),
            pltpu.VMEM((ROWS, D), BF16),
            pltpu.VMEM((ROWS + 2 * HALO, D), BF16),
            pltpu.VMEM((2, HALO, D), BF16),
            pltpu.VMEM((NZ, NX, NC, 32, FL), BF16),
            pltpu.VMEM((NZ, NX, NC, 32, FL), BF16),
            pltpu.VMEM((NZ, NX, NC, 32, FL), BF16),
            pltpu.VMEM((FL, D), BF16),
            pltpu.VMEM((CH, FL), BF16),
            pltpu.VMEM((3, CH, D), BF16),
            pltpu.VMEM((CH, D), F32),
            pltpu.VMEM((2, 128, D), BF16),
            pltpu.VMEM((4, 128, D), BF16),
            pltpu.SemaphoreType.DMA((NSEM,)),
            pltpu.SemaphoreType.DMA((NSEM,)),
            pltpu.SemaphoreType.DMA((NLOC,)),
        ],
        compiler_params=pltpu.CompilerParams(
            collective_id=0, has_side_effects=True, vmem_limit_bytes=62 * 1024 * 1024
        ),
        name="layer",
    )(
        sink,
        jnp.cos(angle),
        jnp.sin(angle),
        query,
        norm_gain.reshape(1, D),
        conv_gate,
        conv_value,
        key.T,
        value.T,
        residual,
        w_out,
        w_gate,
        w_value,
        w_down.T,
    )


def solution(mesh):
    return jax.shard_map(
        shards,
        mesh=mesh,
        in_specs=(
            P("sp", None),
            P("sp", "tp"),
            P("sp", "tp"),
            P("sp", "tp"),
            P("tp"),
            P(),
            P("tp", None),
            P("sp", "tp"),
            P("sp", "tp"),
            P(None, "tp"),
            P(None, "tp"),
            P("tp", "sp"),
        ),
        out_specs=P(("sp", "tp"), None),
        check_vma=False,
    )
```

```python
import functools

import jax
import jax.numpy as jnp
from jax import lax
from jax.experimental import pallas as pl
from jax.experimental.pallas import tpu as pltpu
from jax.sharding import PartitionSpec as P

HD = 64
WINDOW = 128
THETA = 10000.0
EPS = 1e-06
MESH = pl.DeviceIdType.MESH

NZ, NX, NC, NY = 8, 4, 2, 4
ROWS = 1024
D = 2048
FL = 1024
QC = 256
CH = 256
HALO = 16
NSEND = 6
NRECV = 64
NLOC = 12
NT = (((1,), (1,)), ((), ()))
F32 = jnp.float32
BF16 = jnp.bfloat16


class Slot:
    def __init__(self, comm, index):
        self.comm, self.sem = comm, comm.recv.at[index]
        self.size, self.done = 0, False

    def wait_recv(self):
        if not self.done:
            self.done = True
            self.comm.wait(self.sem, self.size)


class Comm:
    def __init__(self, send, recv, local, filler):
        self.send, self.recv, self.local, self.filler = send, recv, local, filler
        self.slots, self.lcount = 0, 0
        self.groups = {}

    def slot(self):
        assert self.slots < NRECV
        self.slots += 1
        return Slot(self, self.slots - 1)

    def wait(self, sem, size):
        view = self.filler.at[0 : size // (2 * D)]
        pltpu.make_async_copy(view, view, sem).wait()

    def start(self, src, dst, slot=None, group="rest", **where):
        slot = slot or self.slot()
        assert not slot.done
        if group not in self.groups:
            assert len(self.groups) < NSEND
            self.groups[group] = [self.send.at[len(self.groups)], 0]
        size = 2
        for extent in src.shape:
            size *= extent
        slot.size += size
        self.groups[group][1] += size
        copy = pltpu.make_async_remote_copy(
            src_ref=src,
            dst_ref=dst,
            send_sem=self.groups[group][0],
            recv_sem=slot.sem,
            device_id=where,
            device_id_type=MESH,
        )
        copy.start()
        return slot

    def here(self, src, dst):
        copy = pltpu.make_async_copy(src, dst, self.local.at[self.lcount])
        self.lcount += 1
        copy.start()
        return copy

    def sent(self):
        for sem, size in self.groups.values():
            self.wait(sem, size)


def turned(x, cosine, sine):
    lane = lax.broadcasted_iota(jnp.int32, x.shape, 1)
    other = jnp.where((lane & 63) < 32, pltpu.roll(x, 96, 1), pltpu.roll(x, 32, 1))
    return x * cosine + other * sine


def layer(
    sink_ref,
    inverse_ref,
    q_hbm,
    gain_hbm,
    tap_gate_hbm,
    tap_value_hbm,
    key_hbm,
    value_hbm,
    res_hbm,
    wo_hbm,
    g_hbm,
    v_hbm,
    d_hbm,
    out_ref,
    cos_ref,
    sin_ref,
    q_ref,
    gain_ref,
    tap_gate,
    tap_value,
    kvx,
    qr,
    ka,
    kb,
    va,
    vb,
    att,
    wo,
    res,
    nrm,
    edge,
    g,
    v,
    d,
    wdown,
    hid,
    part,
    own,
    rin,
    fin,
    send,
    recv,
    local,
):
    s = lax.axis_index("sp")
    t = lax.axis_index("tp")
    nsp = NZ * NX * NC
    z, x, c = s // (NX * NC), (s // NC) % NX, s % NC

    def at(dz, dx, dc=0):
        return (((z + dz + NZ) % NZ) * NX + (x + dx + NX) % NX) * NC + (c + dc) % NC

    def zi(dz):
        return (z + dz + NZ) % NZ

    def xi(dx):
        return (x + dx + NX) % NX

    ahead, behind = (s + 1) % nsp, (s + nsp - 1) % nsp
    mate = at(0, 0, 1)
    ty = [(t + k) % NY for k in range(NY)]

    cm = Comm(send, recv, local, nrm)

    def cell(weight, dz, dx=0):
        return weight.at[zi(dz), xi(dx), c]

    def grow(dz):
        return g.at[zi(dz), :, c]

    l_v, l_d = cm.here(v_hbm, v.at[z, x, c]), cm.here(d_hbm, d.at[z, x, c])
    l_kv = [
        cm.here(key_hbm, kvx.at[0:HD, pl.ds(WINDOW, ROWS)]),
        cm.here(value_hbm, kvx.at[HD : 2 * HD, pl.ds(WINDOW, ROWS)]),
    ]
    l_wo = cm.here(wo_hbm, wo.at[pl.ds(pl.multiple_of(t * QC, QC), QC)])
    l_g = cm.here(g_hbm, g.at[z, x, c])
    l_q = cm.here(q_hbm, q_ref)
    l_small = [cm.here(gain_hbm, gain_ref), cm.here(tap_gate_hbm, tap_gate), cm.here(tap_value_hbm, tap_value)]
    l_res = cm.here(res_hbm, res)

    barrier = pltpu.get_barrier_semaphore()
    peers = [{"sp": i} for i in (ahead, behind, at(1, 0), at(-1, 0), at(0, 1), at(0, 2), at(0, 3), mate)]
    peers += [{"tp": ty[k]} for k in (1, 3)]
    for peer in peers:
        pl.semaphore_signal(barrier, inc=1, device_id=peer, device_id_type=MESH)
    row = lax.broadcasted_iota(jnp.int32, (WINDOW + 16, 128), 0)
    place = jnp.where(row < WINDOW, row, s * ROWS + (row - WINDOW - 1) * WINDOW).astype(F32)
    angle = place * inverse_ref[...]
    cos_ref[...] = jnp.cos(angle)
    sin_ref[...] = jnp.sin(angle)
    pl.semaphore_wait(barrier, len(peers))

    l_v.wait()

    class Flow:
        def __init__(self, weight, group):
            self.weight, self.group = weight, group
            self.ring, self.across, self.on = {}, {}, {}
            self.push = cm.slot()

        def start(self, ref, slot, **where):
            return cm.start(ref, ref, slot, self.group, **where)

        def begin(self):
            own, self.ring[0] = cell(self.weight, 0), cm.slot()
            self.start(own, self.ring[0], sp=at(1, 0))
            self.start(own, self.ring[0], sp=at(-1, 0))

        def share(self, o, dx=0):
            self.start(cell(self.weight, o, dx), self.push, sp=mate)

        def spread(self, o):
            one, self.across[o] = cell(self.weight, o), cm.slot()
            self.start(one, self.across[o], sp=at(0, 1))
            self.start(one, self.across[o], sp=at(0, -1))

        def round(self, k):
            self.ring[k - 1].wait_recv()
            if k < 4:
                low, high = cell(self.weight, -k), cell(self.weight, k)
                if k == 3:
                    low = self.weight.at[zi(-k), x, c, pl.ds(0, 16)]
                    high = self.weight.at[zi(k), x, c, pl.ds(16, 16)]
                self.ring[k] = cm.slot()
                self.start(low, self.ring[k], sp=at(1, 0))
                self.start(high, self.ring[k], sp=at(-1, 0))

        def pass_on(self, o):
            self.across[o].wait_recv()
            if abs(o) not in self.on:
                self.on[abs(o)] = cm.slot()
            if o >= 0:
                self.start(cell(self.weight, o, -1), self.on[abs(o)], sp=at(0, 1))
            else:
                self.start(cell(self.weight, o, 1), self.on[abs(o)], sp=at(0, -1))
            self.share(o, -1)
            self.share(o, 1)

        def last(self, o):
            self.on[abs(o)].wait_recv()
            self.share(o, 2)

        def arrived(self):
            self.push.wait_recv()

    fv, fd = Flow(v, "v"), Flow(d, "d")
    fv.begin()
    fv.spread(0)
    for copy in l_kv:
        copy.wait()
    halo = cm.slot()
    h_low = cm.start(kvx.at[:, pl.ds(ROWS, WINDOW)], kvx.at[:, pl.ds(0, WINDOW)], halo, sp=ahead)
    h_high = cm.start(kvx.at[:, pl.ds(WINDOW, WINDOW)], kvx.at[:, pl.ds(WINDOW + ROWS, WINDOW)], halo, sp=behind)
    l_wo.wait()

    def worows(k, at_row=0, count=128):
        return wo.at[pl.ds(pl.multiple_of(((t + k) % NY) * QC + c * 128 + at_row, 64), count)]

    wo_first, wo_on, wo_push = cm.slot(), cm.slot(), cm.slot()
    cm.start(worows(0), worows(0), wo_first, "wo", tp=ty[1])
    cm.start(worows(0), worows(0), wo_first, "wo", tp=ty[3])
    l_g.wait()
    g_x, g_push = cm.slot(), cm.slot()
    for k in (1, 3, 2):
        cm.start(g.at[z, x, c], g.at[z, x, c], g_x, "g", sp=at(0, k))
    fv.share(0)
    l_d.wait()
    fd.spread(0)

    def table(b):
        base = pl.ds(WINDOW + b, 1)
        cb, sb = cos_ref[base, :], sin_ref[base, :]
        cr, sr = cos_ref[0:WINDOW, :], sin_ref[0:WINDOW, :]
        lane = lax.broadcasted_iota(jnp.int32, (WINDOW, 128), 1)
        sine = sb * cr + cb * sr
        return cb * cr - sb * sr, jnp.where((lane & 63) < 32, -sine, sine)

    def prepare(b, with_query):
        cosine, sine = table(b)
        rows = pl.ds(pl.multiple_of(b * WINDOW, WINDOW), WINDOW)
        if with_query:
            qrows = pl.ds(pl.multiple_of(b * WINDOW - WINDOW, WINDOW), WINDOW)
            for p in range(2):
                lanes = slice(p * 128, p * 128 + 128)
                qr[qrows, lanes] = turned(q_ref[qrows, lanes].astype(F32), cosine, sine).astype(BF16)
        both = kvx[:, rows].astype(F32).T
        lane = lax.broadcasted_iota(jnp.int32, both.shape, 1)
        keys = jnp.where(lane < HD, turned(both, cosine, sine), 0.0)
        values = jnp.where(lane < HD, 0.0, both)
        ka[rows, :] = keys.astype(BF16)
        kb[rows, :] = pltpu.roll(keys, HD, 1).astype(BF16)
        va[rows, :] = pltpu.roll(values, HD, 1).astype(BF16)
        vb[rows, :] = values.astype(BF16)

    l_q.wait()

    @pl.loop(1, ROWS // WINDOW + 1)
    def _(b):
        prepare(b, True)

    h_low.wait_recv()
    h_high.wait_recv()

    @pl.loop(0, 2)
    def _(i):
        prepare(i * (ROWS // WINDOW + 1), False)

    def attend(b):
        start = pl.multiple_of(b * WINDOW, WINDOW)
        rows = pl.ds(start, WINDOW)
        band = pl.ds(start, 3 * WINDOW)
        r = lax.broadcasted_iota(jnp.int32, (WINDOW, 3 * WINDOW), 0)
        j = lax.broadcasted_iota(jnp.int32, (WINDOW, 3 * WINDOW), 1)
        first = s * ROWS + start - WINDOW
        valid = (j >= r) & (j <= r + 2 * WINDOW) & (j + first >= 0) & (j + first < nsp * ROWS)
        lane = lax.broadcasted_iota(jnp.int32, (WINDOW, 128), 1)
        vv = jnp.concatenate([va[band, :], vb[band, :]], axis=0)
        for p in range(2):
            qp = qr[rows, p * 128 : p * 128 + 128]
            weights, inverse = [], []
            for i, keys in enumerate((ka, kb)):
                sc = lax.dot_general(qp, keys[band, :], NT, preferred_element_type=F32)
                sc = jnp.where(valid, sc * HD ** (-0.5), -1e30)
                sink = sink_ref[2 * p + i]
                top = jnp.maximum(jnp.max(sc, axis=1, keepdims=True), sink)
                w = jnp.exp(sc - top)
                denom = jnp.sum(w, axis=1, keepdims=True) + jnp.exp(sink - top)
                weights.append(w.astype(BF16))
                inverse.append(1.0 / denom)
            o = jnp.dot(jnp.concatenate(weights, axis=1), vv, preferred_element_type=F32)
            o = o * jnp.where(lane < HD, inverse[0], inverse[1])
            att[rows, pl.ds(pl.multiple_of(t * QC + p * 128, 128), 128)] = o.astype(BF16)

    def attend_chunk(ci):
        @pl.loop(0, 2)
        def _(i):
            attend(ci * 2 + i)

    a_y, a_on = {}, {}

    def send_att(ci):
        piece = att.at[pl.ds(ci * CH, CH), pl.ds(pl.multiple_of(t * QC, QC), QC)]
        a_y[ci] = cm.slot()
        cm.start(piece, piece, a_y[ci], tp=ty[1])
        cm.start(piece, piece, a_y[ci], tp=ty[3])

    def pass_att(ci):
        a_y[ci].wait_recv()
        a_on[ci] = cm.slot()
        piece = att.at[pl.ds(ci * CH, 128), pl.ds(pl.multiple_of(ty[3] * QC, QC), QC)]
        cm.start(piece, piece, a_on[ci], tp=ty[1])
        piece = att.at[pl.ds(ci * CH + 128, 128), pl.ds(pl.multiple_of(ty[1] * QC, QC), QC)]
        cm.start(piece, piece, a_on[ci], tp=ty[3])

    def pass_wo():
        wo_first.wait_recv()
        cm.start(worows(3, 0, 64), worows(3, 0, 64), wo_on, "wo", tp=ty[1])
        cm.start(worows(1, 64, 64), worows(1, 64, 64), wo_on, "wo", tp=ty[3])
        cm.start(worows(3), worows(3), wo_push, "wo", sp=mate)
        cm.start(worows(1), worows(1), wo_push, "wo", sp=mate)

    def last_wo():
        wo_on.wait_recv()
        cm.start(worows(2), worows(2), wo_push, "wo", sp=mate)

    g_ring = {}

    def g_send(ref, slot, where):
        cm.start(ref, ref, slot, "g", sp=where)

    def g_first():
        g_x.wait_recv()
        g_ring[0] = cm.slot()
        g_send(grow(0), g_ring[0], at(1, 0))
        g_send(grow(0), g_ring[0], at(-1, 0))
        g_send(grow(0), g_push, mate)

    def g_round(k):
        g_ring[k - 1].wait_recv()
        if k < 4:
            low, high = grow(-k), grow(k)
            if k == 3:
                low, high = g.at[zi(-k), pl.ds(0, 2), c], g.at[zi(k), pl.ds(2, 2), c]
            g_ring[k] = cm.slot()
            g_send(low, g_ring[k], at(1, 0))
            g_send(high, g_ring[k], at(-1, 0))
            g_send(grow(k), g_push, mate)
        g_send(grow(-k), g_push, mate)

    def middle(ci):
        a_on[ci].wait_recv()
        rows = pl.ds(ci * CH, CH)
        nrows = pl.ds(HALO + ci * CH, CH)
        total = jnp.zeros((CH, 1), F32)
        for n in range(D // 512):
            cols = slice(n * 512, n * 512 + 512)
            mid = res[rows, cols].astype(F32) + jnp.dot(att[rows, :], wo[:, cols], preferred_element_type=F32)
            mid = mid.astype(BF16)
            res[rows, cols] = mid
            wide = mid.astype(F32)
            total = total + jnp.sum(wide * wide, axis=1, keepdims=True)
        scale = lax.rsqrt(total / D + EPS)
        for n in range(D // 512):
            cols = slice(n * 512, n * 512 + 512)
            nrm[nrows, cols] = (res[rows, cols].astype(F32) * scale * gain_ref[:, cols]).astype(BF16)

    def up(tc):
        rows = pl.ds(pl.multiple_of(tc * CH, CH), CH + 2 * HALO)
        for n in range(FL // 512):
            cols = slice(n * 512, n * 512 + 512)

            def convolved(weight, taps_ref):
                u = jnp.dot(nrm[rows, :], weight.reshape(D, 512), preferred_element_type=F32)
                u = u.astype(BF16).astype(F32)
                taps = taps_ref[:, cols].astype(F32)
                return (
                    u[HALO - 1 : HALO - 1 + CH] * taps[0:1]
                    + u[HALO : HALO + CH] * taps[1:2]
                    + u[HALO + 1 : HALO + 1 + CH] * taps[2:3]
                )

            gate = convolved(g[:, :, :, :, cols], tap_gate)
            value = convolved(v[:, :, :, :, cols], tap_value)
            hid[:, cols] = (gate / (1.0 + jnp.exp(-gate)) * value).astype(BF16)

    def turn_down():
        for n in range(NZ):
            wdown[:, n * 256 : n * 256 + 256] = d[n].reshape(256, FL).T

    def down(into, tiles=range(D // 512)):
        for n in tiles:
            cols = slice(n * 512, n * 512 + 512)
            into[:, cols] = jnp.dot(hid[...], wdown[:, cols], preferred_element_type=F32).astype(into.dtype)

    attend_chunk(0)
    fv.round(1)
    for o in (1, -1):
        fv.spread(o)
        fv.share(o)
    fv.pass_on(0)
    fd.begin()
    attend_chunk(3)
    send_att(0)
    fv.round(2)
    g_first()
    for o in (2, -2):
        fv.spread(o)
        fv.share(o)
    attend_chunk(1)
    send_att(3)
    fd.round(1)
    fd.spread(1)
    fd.spread(-1)
    attend_chunk(2)
    fv.pass_on(1)
    fv.pass_on(-1)
    fd.pass_on(0)
    fv.last(0)
    fv.round(3)
    for o in (3, -3):
        fv.spread(o)
        fv.share(o)
    pass_wo()
    send_att(1)
    send_att(2)
    fd.round(2)
    g_round(1)
    fv.round(4)
    fv.spread(-4)
    fv.share(-4)
    fd.spread(2)
    fd.spread(-2)
    fv.pass_on(2)
    fv.pass_on(-2)
    fv.last(1)
    fv.last(-1)
    fd.share(0)
    pass_att(0)
    pass_att(3)
    fd.pass_on(1)
    fd.pass_on(-1)
    fd.round(3)
    fd.spread(3)
    fd.spread(-3)
    last_wo()
    fv.pass_on(3)
    fv.pass_on(-3)
    fv.pass_on(-4)
    pass_att(1)
    g_round(2)
    fd.round(4)
    fd.spread(-4)
    pass_att(2)
    for copy in [l_res] + l_small:
        copy.wait()
    fv.last(2)
    fv.last(-2)
    for o in (1, -1, 2, -2):
        fd.share(o)
    wo_push.wait_recv()
    middle(0)
    fd.pass_on(2)
    fd.pass_on(-2)
    middle(3)
    g_round(3)
    e_both = cm.slot()
    cm.start(nrm.at[pl.ds(HALO, HALO)], edge.at[1], e_both, sp=behind)
    fd.pass_on(3)
    fd.pass_on(-3)
    fd.pass_on(-4)
    middle(1)
    cm.start(nrm.at[pl.ds(ROWS, HALO)], edge.at[0], e_both, sp=ahead)
    for o in (3, -3, -4):
        fv.last(o)
    for o in (0, 1, -1, 2, -2):
        fd.last(o)
    middle(2)
    g_round(4)
    for o in (3, -3, -4):
        fd.share(o)
        fd.last(o)
    fv.arrived()
    g_push.wait_recv()
    e_both.wait_recv()
    nrm[0:HALO, :] = jnp.where(s > 0, edge[0].astype(F32), 0.0).astype(BF16)
    nrm[HALO + ROWS :, :] = jnp.where(s < nsp - 1, edge[1].astype(F32), 0.0).astype(BF16)
    fd.arrived()
    turn_down()
    up(ty[2])
    sides = (slice(0, D // 2), slice(D // 2, D))
    s_both = []
    for i, side in enumerate(sides):
        down(part.at[0], (2 * i, 2 * i + 1))
        s_both.append(cm.slot())
        cm.start(part.at[0, 0:128, side], rin.at[0, :, side], s_both[i], "sum", tp=ty[1])
        cm.start(part.at[0, 128:256, side], rin.at[1, :, side], s_both[i], "sum", tp=ty[3])
    up(ty[1])
    down(part.at[1])
    direct = cm.slot()
    cm.start(part.at[1, 128:256], fin.at[1], direct, "sum", tp=ty[1])
    up(ty[3])
    down(part.at[2])
    cm.start(part.at[2, 0:128], fin.at[2], direct, "sum", tp=ty[3])

    def joined(which, rows, side):
        base = 0 if side.start == 0 else D // 2

        @pl.loop(0, 4)
        def _(n):
            cols = pl.ds(pl.multiple_of(base + n * 256, 256), 256)
            total = part[1 + which, rows, cols].astype(F32) + rin[which, :, cols].astype(F32)
            part[1 + which, rows, cols] = total.astype(BF16)

    f_both = []
    for i, side in enumerate(sides):
        s_both[i].wait_recv()
        f_both.append(cm.slot())
        joined(0, slice(0, 128), side)
        cm.start(part.at[1, 0:128, side], fin.at[0, :, side], f_both[i], "sum", tp=ty[1])
        joined(1, slice(128, 256), side)
        cm.start(part.at[2, 128:256, side], fin.at[3, :, side], f_both[i], "sum", tp=ty[3])
    up(t)
    down(own)
    direct.wait_recv()
    for i, side in enumerate(sides):
        f_both[i].wait_recv()

        @pl.loop(4 * i, 4 * i + 4)
        def _(n):
            cols = pl.ds(pl.multiple_of(n * 256, 256), 256)
            for k in range(2):
                rows = slice(k * 128, k * 128 + 128)
                mrows = pl.ds(pl.multiple_of(t * CH + k * 128, 128), 128)
                ffn = own[rows, cols] + fin[k, :, cols].astype(F32) + fin[2 + k, :, cols].astype(F32)
                out_ref[rows, cols] = (res[mrows, cols].astype(F32) + ffn).astype(BF16)

    cm.sent()


def shards(
    residual,
    query,
    key,
    value,
    sink,
    norm_gain,
    w_out,
    w_gate,
    w_value,
    conv_gate,
    conv_value,
    w_down,
):
    inverse = 1.0 / THETA ** (jnp.arange(0, HD, 2, dtype=F32) / HD)
    vmem = pl.BlockSpec(memory_space=pltpu.VMEM)
    hbm = pl.BlockSpec(memory_space=pl.ANY)
    return pl.pallas_call(
        layer,
        out_shape=jax.ShapeDtypeStruct((CH, D), BF16),
        in_specs=[pl.BlockSpec(memory_space=pltpu.SMEM)] + [vmem] + [hbm] * 11,
        out_specs=vmem,
        scratch_shapes=[
            pltpu.VMEM((WINDOW + 16, 128), F32),
            pltpu.VMEM((WINDOW + 16, 128), F32),
            pltpu.VMEM((ROWS, QC), BF16),
            pltpu.VMEM((1, D), F32),
            pltpu.VMEM((3, FL), BF16),
            pltpu.VMEM((3, FL), BF16),
            pltpu.VMEM((2 * HD, ROWS + 2 * WINDOW), BF16),
            pltpu.VMEM((ROWS, QC), BF16),
            pltpu.VMEM((ROWS + 2 * WINDOW, 128), BF16),
            pltpu.VMEM((ROWS + 2 * WINDOW, 128), BF16),
            pltpu.VMEM((ROWS + 2 * WINDOW, 128), BF16),
            pltpu.VMEM((ROWS + 2 * WINDOW, 128), BF16),
            pltpu.VMEM((ROWS, NY * QC), BF16),
            pltpu.VMEM((NY * QC, D), BF16),
            pltpu.VMEM((ROWS, D), BF16),
            pltpu.VMEM((ROWS + 2 * HALO, D), BF16),
            pltpu.VMEM((2, HALO, D), BF16),
            pltpu.VMEM((NZ, NX, NC, 32, FL), BF16),
            pltpu.VMEM((NZ, NX, NC, 32, FL), BF16),
            pltpu.VMEM((NZ, NX, NC, 32, FL), BF16),
            pltpu.VMEM((FL, D), BF16),
            pltpu.VMEM((CH, FL), BF16),
            pltpu.VMEM((3, CH, D), BF16),
            pltpu.VMEM((CH, D), F32),
            pltpu.VMEM((2, 128, D), BF16),
            pltpu.VMEM((4, 128, D), BF16),
            pltpu.SemaphoreType.DMA((NSEND,)),
            pltpu.SemaphoreType.DMA((NRECV,)),
            pltpu.SemaphoreType.DMA((NLOC,)),
        ],
        compiler_params=pltpu.CompilerParams(
            collective_id=0, has_side_effects=True, vmem_limit_bytes=62 * 1024 * 1024
        ),
        name="layer",
    )(
        sink,
        jnp.tile(inverse, 4).reshape(1, 128),
        query,
        norm_gain.reshape(1, D),
        conv_gate,
        conv_value,
        key.T,
        value.T,
        residual,
        w_out,
        w_gate,
        w_value,
        w_down.T,
    )


def solution(mesh):
    return jax.shard_map(
        shards,
        mesh=mesh,
        in_specs=(
            P("sp", None),
            P("sp", "tp"),
            P("sp", "tp"),
            P("sp", "tp"),
            P("tp"),
            P(),
            P("tp", None),
            P("sp", "tp"),
            P("sp", "tp"),
            P(None, "tp"),
            P(None, "tp"),
            P("tp", "sp"),
        ),
        out_specs=P(("sp", "tp"), None),
        check_vma=False,
    )
```

```python
import functools

import jax
import jax.numpy as jnp
from jax import lax
from jax.experimental import pallas as pl
from jax.experimental.pallas import tpu as pltpu
from jax.sharding import PartitionSpec as P

HD = 64
WINDOW = 128
THETA = 10000.0
EPS = 1e-06
MESH = pl.DeviceIdType.MESH

NZ, NX, NC, NY = 8, 4, 2, 4
ROWS = 1024
D = 2048
FL = 1024
QC = 256
CH = 256
HALO = 16
NSEND = 6
NRECV = 64
NLOC = 14
NT = (((1,), (1,)), ((), ()))
F32 = jnp.float32
BF16 = jnp.bfloat16


class Slot:
    def __init__(self, comm, index):
        self.comm, self.sem = comm, comm.recv.at[index]
        self.size, self.done = 0, False

    def wait_recv(self):
        if not self.done:
            self.done = True
            self.comm.wait(self.sem, self.size)


class Comm:
    def __init__(self, send, recv, local, filler):
        self.send, self.recv, self.local, self.filler = send, recv, local, filler
        self.slots, self.lcount = 0, 0
        self.groups = {}

    def slot(self):
        assert self.slots < NRECV
        self.slots += 1
        return Slot(self, self.slots - 1)

    def wait(self, sem, size):
        view = self.filler.at[0 : size // (2 * D)]
        pltpu.make_async_copy(view, view, sem).wait()

    def start(self, src, dst, slot=None, group="rest", **where):
        slot = slot or self.slot()
        assert not slot.done
        if group not in self.groups:
            assert len(self.groups) < NSEND
            self.groups[group] = [self.send.at[len(self.groups)], 0]
        size = 2
        for extent in src.shape:
            size *= extent
        slot.size += size
        self.groups[group][1] += size
        copy = pltpu.make_async_remote_copy(
            src_ref=src,
            dst_ref=dst,
            send_sem=self.groups[group][0],
            recv_sem=slot.sem,
            device_id=where,
            device_id_type=MESH,
        )
        copy.start()
        return slot

    def here(self, src, dst):
        copy = pltpu.make_async_copy(src, dst, self.local.at[self.lcount])
        self.lcount += 1
        copy.start()
        return copy

    def sent(self):
        for sem, size in self.groups.values():
            self.wait(sem, size)


def turned(x, cosine, sine):
    lane = lax.broadcasted_iota(jnp.int32, x.shape, 1)
    other = jnp.where((lane & 63) < 32, pltpu.roll(x, 96, 1), pltpu.roll(x, 32, 1))
    return x * cosine + other * sine


def layer(
    sink_ref,
    inverse_ref,
    q_hbm,
    gain_hbm,
    tap_gate_hbm,
    tap_value_hbm,
    key_hbm,
    value_hbm,
    res_hbm,
    wo_hbm,
    g_hbm,
    v_hbm,
    d_hbm,
    out_hbm,
    cos_ref,
    sin_ref,
    q_ref,
    gain_ref,
    tap_gate,
    tap_value,
    kvx,
    qr,
    ka,
    kb,
    va,
    vb,
    att,
    wo,
    res,
    nrm,
    edge,
    g,
    v,
    d,
    wdown,
    hid,
    part,
    own,
    rin,
    fin,
    send,
    recv,
    local,
):
    s = lax.axis_index("sp")
    t = lax.axis_index("tp")
    nsp = NZ * NX * NC
    z, x, c = s // (NX * NC), (s // NC) % NX, s % NC

    def at(dz, dx, dc=0):
        return (((z + dz + NZ) % NZ) * NX + (x + dx + NX) % NX) * NC + (c + dc) % NC

    def zi(dz):
        return (z + dz + NZ) % NZ

    def xi(dx):
        return (x + dx + NX) % NX

    ahead, behind = (s + 1) % nsp, (s + nsp - 1) % nsp
    mate = at(0, 0, 1)
    ty = [(t + k) % NY for k in range(NY)]

    cm = Comm(send, recv, local, nrm)

    def cell(weight, dz, dx=0):
        return weight.at[zi(dz), xi(dx), c]

    def grow(dz):
        return g.at[zi(dz), :, c]

    l_v, l_d = cm.here(v_hbm, v.at[z, x, c]), cm.here(d_hbm, d.at[z, x, c])
    l_kv = [
        cm.here(key_hbm, kvx.at[0:HD, pl.ds(WINDOW, ROWS)]),
        cm.here(value_hbm, kvx.at[HD : 2 * HD, pl.ds(WINDOW, ROWS)]),
    ]
    l_wo = cm.here(wo_hbm, wo.at[pl.ds(pl.multiple_of(t * QC, QC), QC)])
    l_g = cm.here(g_hbm, g.at[z, x, c])
    l_q = cm.here(q_hbm, q_ref)
    l_small = [cm.here(gain_hbm, gain_ref), cm.here(tap_gate_hbm, tap_gate), cm.here(tap_value_hbm, tap_value)]
    l_res = cm.here(res_hbm, res)

    barrier = pltpu.get_barrier_semaphore()
    peers = [{"sp": i} for i in (ahead, behind, at(1, 0), at(-1, 0), at(0, 1), at(0, 2), at(0, 3), mate)]
    peers += [{"tp": ty[k]} for k in (1, 3)]
    for peer in peers:
        pl.semaphore_signal(barrier, inc=1, device_id=peer, device_id_type=MESH)
    row = lax.broadcasted_iota(jnp.int32, (WINDOW + 16, 128), 0)
    place = jnp.where(row < WINDOW, row, s * ROWS + (row - WINDOW - 1) * WINDOW).astype(F32)
    angle = place * inverse_ref[...]
    cos_ref[...] = jnp.cos(angle)
    sin_ref[...] = jnp.sin(angle)
    pl.semaphore_wait(barrier, len(peers))

    l_v.wait()

    class Flow:
        def __init__(self, weight, group):
            self.weight, self.group = weight, group
            self.ring, self.across, self.on = {}, {}, {}
            self.push = cm.slot()

        def start(self, ref, slot, **where):
            return cm.start(ref, ref, slot, self.group, **where)

        def begin(self):
            own, self.ring[0] = cell(self.weight, 0), cm.slot()
            self.start(own, self.ring[0], sp=at(1, 0))
            self.start(own, self.ring[0], sp=at(-1, 0))

        def share(self, o, dx=0):
            self.start(cell(self.weight, o, dx), self.push, sp=mate)

        def spread(self, o):
            one, self.across[o] = cell(self.weight, o), cm.slot()
            self.start(one, self.across[o], sp=at(0, 1))
            self.start(one, self.across[o], sp=at(0, -1))

        def round(self, k):
            self.ring[k - 1].wait_recv()
            if k < 4:
                low, high = cell(self.weight, -k), cell(self.weight, k)
                if k == 3:
                    low = self.weight.at[zi(-k), x, c, pl.ds(0, 16)]
                    high = self.weight.at[zi(k), x, c, pl.ds(16, 16)]
                self.ring[k] = cm.slot()
                self.start(low, self.ring[k], sp=at(1, 0))
                self.start(high, self.ring[k], sp=at(-1, 0))

        def pass_on(self, o):
            self.across[o].wait_recv()
            if abs(o) not in self.on:
                self.on[abs(o)] = cm.slot()
            if o >= 0:
                self.start(cell(self.weight, o, -1), self.on[abs(o)], sp=at(0, 1))
            else:
                self.start(cell(self.weight, o, 1), self.on[abs(o)], sp=at(0, -1))
            self.share(o, -1)
            self.share(o, 1)

        def last(self, o):
            self.on[abs(o)].wait_recv()
            self.share(o, 2)

        def arrived(self):
            self.push.wait_recv()

    fv, fd = Flow(v, "v"), Flow(d, "d")
    fv.begin()
    fv.spread(0)
    for copy in l_kv:
        copy.wait()
    halo = cm.slot()
    h_low = cm.start(kvx.at[:, pl.ds(ROWS, WINDOW)], kvx.at[:, pl.ds(0, WINDOW)], halo, sp=ahead)
    h_high = cm.start(kvx.at[:, pl.ds(WINDOW, WINDOW)], kvx.at[:, pl.ds(WINDOW + ROWS, WINDOW)], halo, sp=behind)
    l_wo.wait()

    def worows(k, at_row=0, count=128):
        return wo.at[pl.ds(pl.multiple_of(((t + k) % NY) * QC + c * 128 + at_row, 64), count)]

    wo_first, wo_on, wo_push = cm.slot(), cm.slot(), cm.slot()
    cm.start(worows(0), worows(0), wo_first, "wo", tp=ty[1])
    cm.start(worows(0), worows(0), wo_first, "wo", tp=ty[3])
    l_g.wait()
    g_x, g_push = cm.slot(), cm.slot()
    for k in (1, 3, 2):
        cm.start(g.at[z, x, c], g.at[z, x, c], g_x, "g", sp=at(0, k))
    fv.share(0)
    l_d.wait()
    fd.spread(0)

    def table(b):
        base = pl.ds(WINDOW + b, 1)
        cb, sb = cos_ref[base, :], sin_ref[base, :]
        cr, sr = cos_ref[0:WINDOW, :], sin_ref[0:WINDOW, :]
        lane = lax.broadcasted_iota(jnp.int32, (WINDOW, 128), 1)
        sine = sb * cr + cb * sr
        return cb * cr - sb * sr, jnp.where((lane & 63) < 32, -sine, sine)

    def prepare(b, with_query):
        cosine, sine = table(b)
        rows = pl.ds(pl.multiple_of(b * WINDOW, WINDOW), WINDOW)
        if with_query:
            qrows = pl.ds(pl.multiple_of(b * WINDOW - WINDOW, WINDOW), WINDOW)
            for p in range(2):
                lanes = slice(p * 128, p * 128 + 128)
                qr[qrows, lanes] = turned(q_ref[qrows, lanes].astype(F32), cosine, sine).astype(BF16)
        both = kvx[:, rows].astype(F32).T
        lane = lax.broadcasted_iota(jnp.int32, both.shape, 1)
        keys = jnp.where(lane < HD, turned(both, cosine, sine), 0.0)
        values = jnp.where(lane < HD, 0.0, both)
        ka[rows, :] = keys.astype(BF16)
        kb[rows, :] = pltpu.roll(keys, HD, 1).astype(BF16)
        va[rows, :] = pltpu.roll(values, HD, 1).astype(BF16)
        vb[rows, :] = values.astype(BF16)

    l_q.wait()

    @pl.loop(1, ROWS // WINDOW + 1)
    def _(b):
        prepare(b, True)

    h_low.wait_recv()
    h_high.wait_recv()

    @pl.loop(0, 2)
    def _(i):
        prepare(i * (ROWS // WINDOW + 1), False)

    def attend(b):
        start = pl.multiple_of(b * WINDOW, WINDOW)
        rows = pl.ds(start, WINDOW)
        band = pl.ds(start, 3 * WINDOW)
        r = lax.broadcasted_iota(jnp.int32, (WINDOW, 3 * WINDOW), 0)
        j = lax.broadcasted_iota(jnp.int32, (WINDOW, 3 * WINDOW), 1)
        first = s * ROWS + start - WINDOW
        valid = (j >= r) & (j <= r + 2 * WINDOW) & (j + first >= 0) & (j + first < nsp * ROWS)
        lane = lax.broadcasted_iota(jnp.int32, (WINDOW, 128), 1)
        vv = jnp.concatenate([va[band, :], vb[band, :]], axis=0)
        for p in range(2):
            qp = qr[rows, p * 128 : p * 128 + 128]
            weights, inverse = [], []
            for i, keys in enumerate((ka, kb)):
                sc = lax.dot_general(qp, keys[band, :], NT, preferred_element_type=F32)
                sc = jnp.where(valid, sc * HD ** (-0.5), -1e30)
                sink = sink_ref[2 * p + i]
                top = jnp.maximum(jnp.max(sc, axis=1, keepdims=True), sink)
                w = jnp.exp(sc - top)
                denom = jnp.sum(w, axis=1, keepdims=True) + jnp.exp(sink - top)
                weights.append(w.astype(BF16))
                inverse.append(1.0 / denom)
            o = jnp.dot(jnp.concatenate(weights, axis=1), vv, preferred_element_type=F32)
            o = o * jnp.where(lane < HD, inverse[0], inverse[1])
            att[rows, pl.ds(pl.multiple_of(t * QC + p * 128, 128), 128)] = o.astype(BF16)

    def attend_chunk(ci):
        @pl.loop(0, 2)
        def _(i):
            attend(ci * 2 + i)

    a_y, a_on = {}, {}

    def send_att(ci):
        piece = att.at[pl.ds(ci * CH, CH), pl.ds(pl.multiple_of(t * QC, QC), QC)]
        a_y[ci] = cm.slot()
        cm.start(piece, piece, a_y[ci], tp=ty[1])
        cm.start(piece, piece, a_y[ci], tp=ty[3])

    def pass_att(ci):
        a_y[ci].wait_recv()
        a_on[ci] = cm.slot()
        piece = att.at[pl.ds(ci * CH, 128), pl.ds(pl.multiple_of(ty[3] * QC, QC), QC)]
        cm.start(piece, piece, a_on[ci], tp=ty[1])
        piece = att.at[pl.ds(ci * CH + 128, 128), pl.ds(pl.multiple_of(ty[1] * QC, QC), QC)]
        cm.start(piece, piece, a_on[ci], tp=ty[3])

    def pass_wo():
        wo_first.wait_recv()
        cm.start(worows(3, 0, 64), worows(3, 0, 64), wo_on, "wo", tp=ty[1])
        cm.start(worows(1, 64, 64), worows(1, 64, 64), wo_on, "wo", tp=ty[3])
        cm.start(worows(3), worows(3), wo_push, "wo", sp=mate)
        cm.start(worows(1), worows(1), wo_push, "wo", sp=mate)

    def last_wo():
        wo_on.wait_recv()
        cm.start(worows(2), worows(2), wo_push, "wo", sp=mate)

    g_ring = {}

    def g_send(ref, slot, where):
        cm.start(ref, ref, slot, "g", sp=where)

    def g_first():
        g_x.wait_recv()
        g_ring[0] = cm.slot()
        g_send(grow(0), g_ring[0], at(1, 0))
        g_send(grow(0), g_ring[0], at(-1, 0))
        g_send(grow(0), g_push, mate)

    def g_round(k):
        g_ring[k - 1].wait_recv()
        if k < 4:
            low, high = grow(-k), grow(k)
            if k == 3:
                low, high = g.at[zi(-k), pl.ds(0, 2), c], g.at[zi(k), pl.ds(2, 2), c]
            g_ring[k] = cm.slot()
            g_send(low, g_ring[k], at(1, 0))
            g_send(high, g_ring[k], at(-1, 0))
            g_send(grow(k), g_push, mate)
        g_send(grow(-k), g_push, mate)

    def middle(ci):
        a_on[ci].wait_recv()
        rows = pl.ds(ci * CH, CH)
        nrows = pl.ds(HALO + ci * CH, CH)
        total = jnp.zeros((CH, 1), F32)
        for n in range(D // 512):
            cols = slice(n * 512, n * 512 + 512)
            mid = res[rows, cols].astype(F32) + jnp.dot(att[rows, :], wo[:, cols], preferred_element_type=F32)
            mid = mid.astype(BF16)
            res[rows, cols] = mid
            wide = mid.astype(F32)
            total = total + jnp.sum(wide * wide, axis=1, keepdims=True)
        scale = lax.rsqrt(total / D + EPS)
        for n in range(D // 512):
            cols = slice(n * 512, n * 512 + 512)
            nrm[nrows, cols] = (res[rows, cols].astype(F32) * scale * gain_ref[:, cols]).astype(BF16)

    def up(tc):
        rows = pl.ds(pl.multiple_of(tc * CH, CH), CH + 2 * HALO)
        for n in range(FL // 512):
            cols = slice(n * 512, n * 512 + 512)

            def convolved(weight, taps_ref):
                u = jnp.dot(nrm[rows, :], weight.reshape(D, 512), preferred_element_type=F32)
                u = u.astype(BF16).astype(F32)
                taps = taps_ref[:, cols].astype(F32)
                return (
                    u[HALO - 1 : HALO - 1 + CH] * taps[0:1]
                    + u[HALO : HALO + CH] * taps[1:2]
                    + u[HALO + 1 : HALO + 1 + CH] * taps[2:3]
                )

            gate = convolved(g[:, :, :, :, cols], tap_gate)
            value = convolved(v[:, :, :, :, cols], tap_value)
            hid[:, cols] = (gate / (1.0 + jnp.exp(-gate)) * value).astype(BF16)

    def turn_down():
        for n in range(NZ):
            wdown[:, n * 256 : n * 256 + 256] = d[n].reshape(256, FL).T

    def down(into, tiles=range(D // 512)):
        for n in tiles:
            cols = slice(n * 512, n * 512 + 512)
            into[:, cols] = jnp.dot(hid[...], wdown[:, cols], preferred_element_type=F32).astype(into.dtype)

    attend_chunk(0)
    fv.round(1)
    for o in (1, -1):
        fv.spread(o)
        fv.share(o)
    fv.pass_on(0)
    fd.begin()
    attend_chunk(3)
    send_att(0)
    fv.round(2)
    g_first()
    for o in (2, -2):
        fv.spread(o)
        fv.share(o)
    attend_chunk(1)
    send_att(3)
    fd.round(1)
    fd.spread(1)
    fd.spread(-1)
    attend_chunk(2)
    fv.pass_on(1)
    fv.pass_on(-1)
    fd.pass_on(0)
    fv.last(0)
    fv.round(3)
    for o in (3, -3):
        fv.spread(o)
        fv.share(o)
    pass_wo()
    send_att(1)
    send_att(2)
    fd.round(2)
    g_round(1)
    fv.round(4)
    fv.spread(-4)
    fv.share(-4)
    fd.spread(2)
    fd.spread(-2)
    fv.pass_on(2)
    fv.pass_on(-2)
    fv.last(1)
    fv.last(-1)
    fd.share(0)
    pass_att(0)
    pass_att(3)
    fd.pass_on(1)
    fd.pass_on(-1)
    fd.round(3)
    fd.spread(3)
    fd.spread(-3)
    last_wo()
    fv.pass_on(3)
    fv.pass_on(-3)
    fv.pass_on(-4)
    pass_att(1)
    g_round(2)
    fd.round(4)
    fd.spread(-4)
    pass_att(2)
    for copy in [l_res] + l_small:
        copy.wait()
    fv.last(2)
    fv.last(-2)
    for o in (1, -1, 2, -2):
        fd.share(o)
    wo_push.wait_recv()
    middle(0)
    fd.pass_on(2)
    fd.pass_on(-2)
    middle(3)
    g_round(3)
    e_both = cm.slot()
    cm.start(nrm.at[pl.ds(HALO, HALO)], edge.at[1], e_both, sp=behind)
    middle(1)
    cm.start(nrm.at[pl.ds(ROWS, HALO)], edge.at[0], e_both, sp=ahead)
    fd.pass_on(3)
    fd.pass_on(-3)
    fd.pass_on(-4)
    for o in (3, -3, -4):
        fv.last(o)
    middle(2)
    g_round(4)
    for o in (0, 1, -1, 2, -2):
        fd.last(o)
    fv.arrived()
    g_push.wait_recv()
    e_both.wait_recv()
    nrm[0:HALO, :] = jnp.where(s > 0, edge[0].astype(F32), 0.0).astype(BF16)
    nrm[HALO + ROWS :, :] = jnp.where(s < nsp - 1, edge[1].astype(F32), 0.0).astype(BF16)
    for o in (3, -3, -4):
        fd.share(o)
        fd.last(o)
    up(ty[2])
    fd.arrived()
    turn_down()
    sides = (slice(0, D // 2), slice(D // 2, D))
    s_both = []
    for i, side in enumerate(sides):
        down(part.at[0], (2 * i, 2 * i + 1))
        s_both.append(cm.slot())
        cm.start(part.at[0, 0:128, side], rin.at[0, :, side], s_both[i], "sum", tp=ty[1])
        cm.start(part.at[0, 128:256, side], rin.at[1, :, side], s_both[i], "sum", tp=ty[3])
    up(ty[1])
    down(part.at[1])
    direct = cm.slot()
    cm.start(part.at[1, 128:256], fin.at[1], direct, "sum", tp=ty[1])
    up(ty[3])
    down(part.at[2])
    cm.start(part.at[2, 0:128], fin.at[2], direct, "sum", tp=ty[3])

    def joined(which, rows, side):
        base = 0 if side.start == 0 else D // 2

        @pl.loop(0, 4)
        def _(n):
            cols = pl.ds(pl.multiple_of(base + n * 256, 256), 256)
            total = part[1 + which, rows, cols].astype(F32) + rin[which, :, cols].astype(F32)
            part[1 + which, rows, cols] = total.astype(BF16)

    f_both = []
    for i, side in enumerate(sides):
        s_both[i].wait_recv()
        f_both.append(cm.slot())
        joined(0, slice(0, 128), side)
        cm.start(part.at[1, 0:128, side], fin.at[0, :, side], f_both[i], "sum", tp=ty[1])
        joined(1, slice(128, 256), side)
        cm.start(part.at[2, 128:256, side], fin.at[3, :, side], f_both[i], "sum", tp=ty[3])
    up(t)
    down(own)
    direct.wait_recv()
    written = []
    for i, side in enumerate(sides):
        f_both[i].wait_recv()

        @pl.loop(4 * i, 4 * i + 4)
        def _(n):
            cols = pl.ds(pl.multiple_of(n * 256, 256), 256)
            for k in range(2):
                rows = slice(k * 128, k * 128 + 128)
                mrows = pl.ds(pl.multiple_of(t * CH + k * 128, 128), 128)
                ffn = own[rows, cols] + fin[k, :, cols].astype(F32) + fin[2 + k, :, cols].astype(F32)
                own[rows, cols] = res[mrows, cols].astype(F32) + ffn

        written.append(cm.here(own.at[:, side], out_hbm.at[:, side]))

    cm.sent()
    for copy in written:
        copy.wait()


def shards(
    residual,
    query,
    key,
    value,
    sink,
    norm_gain,
    w_out,
    w_gate,
    w_value,
    conv_gate,
    conv_value,
    w_down,
):
    pair = (jnp.arange(128, dtype=jnp.int32) % (HD // 2) * 2).astype(F32)
    inverse = 1.0 / THETA ** (pair / HD)
    vmem = pl.BlockSpec(memory_space=pltpu.VMEM)
    hbm = pl.BlockSpec(memory_space=pl.ANY)
    total = pl.pallas_call(
        layer,
        out_shape=jax.ShapeDtypeStruct((CH, D), F32),
        in_specs=[pl.BlockSpec(memory_space=pltpu.SMEM)] + [vmem] + [hbm] * 11,
        out_specs=hbm,
        scratch_shapes=[
            pltpu.VMEM((WINDOW + 16, 128), F32),
            pltpu.VMEM((WINDOW + 16, 128), F32),
            pltpu.VMEM((ROWS, QC), BF16),
            pltpu.VMEM((1, D), F32),
            pltpu.VMEM((3, FL), BF16),
            pltpu.VMEM((3, FL), BF16),
            pltpu.VMEM((2 * HD, ROWS + 2 * WINDOW), BF16),
            pltpu.VMEM((ROWS, QC), BF16),
            pltpu.VMEM((ROWS + 2 * WINDOW, 128), BF16),
            pltpu.VMEM((ROWS + 2 * WINDOW, 128), BF16),
            pltpu.VMEM((ROWS + 2 * WINDOW, 128), BF16),
            pltpu.VMEM((ROWS + 2 * WINDOW, 128), BF16),
            pltpu.VMEM((ROWS, NY * QC), BF16),
            pltpu.VMEM((NY * QC, D), BF16),
            pltpu.VMEM((ROWS, D), BF16),
            pltpu.VMEM((ROWS + 2 * HALO, D), BF16),
            pltpu.VMEM((2, HALO, D), BF16),
            pltpu.VMEM((NZ, NX, NC, 32, FL), BF16),
            pltpu.VMEM((NZ, NX, NC, 32, FL), BF16),
            pltpu.VMEM((NZ, NX, NC, 32, FL), BF16),
            pltpu.VMEM((FL, D), BF16),
            pltpu.VMEM((CH, FL), BF16),
            pltpu.VMEM((3, CH, D), BF16),
            pltpu.VMEM((CH, D), F32),
            pltpu.VMEM((2, 128, D), BF16),
            pltpu.VMEM((4, 128, D), BF16),
            pltpu.SemaphoreType.DMA((NSEND,)),
            pltpu.SemaphoreType.DMA((NRECV,)),
            pltpu.SemaphoreType.DMA((NLOC,)),
        ],
        compiler_params=pltpu.CompilerParams(
            collective_id=0, has_side_effects=True, vmem_limit_bytes=62 * 1024 * 1024
        ),
        name="layer",
    )(
        sink,
        inverse.reshape(1, 128),
        query,
        norm_gain.reshape(1, D),
        conv_gate,
        conv_value,
        key.T,
        value.T,
        residual,
        w_out,
        w_gate,
        w_value,
        w_down.T,
    )
    return total.astype(BF16)


def solution(mesh):
    return jax.shard_map(
        shards,
        mesh=mesh,
        in_specs=(
            P("sp", None),
            P("sp", "tp"),
            P("sp", "tp"),
            P("sp", "tp"),
            P("tp"),
            P(),
            P("tp", None),
            P("sp", "tp"),
            P("sp", "tp"),
            P(None, "tp"),
            P(None, "tp"),
            P("tp", "sp"),
        ),
        out_specs=P(("sp", "tp"), None),
        check_vma=False,
    )
```

```python
import functools

import jax
import jax.numpy as jnp
from jax import lax
from jax.experimental import pallas as pl
from jax.experimental.pallas import tpu as pltpu
from jax.sharding import PartitionSpec as P

HD = 64
WINDOW = 128
THETA = 10000.0
EPS = 1e-06
MESH = pl.DeviceIdType.MESH

NZ, NX, NC, NY = 8, 4, 2, 4
ROWS = 1024
D = 2048
FL = 1024
QC = 256
CH = 256
HALO = 16
NSEND = 6
NRECV = 64
NLOC = 14
NT = (((1,), (1,)), ((), ()))
F32 = jnp.float32
BF16 = jnp.bfloat16


class Slot:
    def __init__(self, comm, index):
        self.comm, self.sem = comm, comm.recv.at[index]
        self.size, self.done = 0, False

    def wait_recv(self):
        if not self.done:
            self.done = True
            self.comm.wait(self.sem, self.size)


class Comm:
    def __init__(self, send, recv, local, filler):
        self.send, self.recv, self.local, self.filler = send, recv, local, filler
        self.slots, self.lcount = 0, 0
        self.groups = {}

    def slot(self):
        assert self.slots < NRECV
        self.slots += 1
        return Slot(self, self.slots - 1)

    def wait(self, sem, size):
        view = self.filler.at[0 : size // (2 * D)]
        pltpu.make_async_copy(view, view, sem).wait()

    def start(self, src, dst, slot=None, group="rest", **where):
        slot = slot or self.slot()
        assert not slot.done
        if group not in self.groups:
            assert len(self.groups) < NSEND
            self.groups[group] = [self.send.at[len(self.groups)], 0]
        size = 2
        for extent in src.shape:
            size *= extent
        slot.size += size
        self.groups[group][1] += size
        copy = pltpu.make_async_remote_copy(
            src_ref=src,
            dst_ref=dst,
            send_sem=self.groups[group][0],
            recv_sem=slot.sem,
            device_id=where,
            device_id_type=MESH,
        )
        copy.start()
        return slot

    def here(self, src, dst):
        copy = pltpu.make_async_copy(src, dst, self.local.at[self.lcount])
        self.lcount += 1
        copy.start()
        return copy

    def sent(self):
        for sem, size in self.groups.values():
            self.wait(sem, size)


def turned(x, cosine, sine):
    lane = lax.broadcasted_iota(jnp.int32, x.shape, 1)
    other = jnp.where((lane & 63) < 32, pltpu.roll(x, 96, 1), pltpu.roll(x, 32, 1))
    return x * cosine + other * sine


def layer(
    sink_ref,
    inverse_ref,
    q_hbm,
    gain_hbm,
    tap_gate_hbm,
    tap_value_hbm,
    key_hbm,
    value_hbm,
    res_hbm,
    wo_hbm,
    g_hbm,
    v_hbm,
    d_hbm,
    out_hbm,
    cos_ref,
    sin_ref,
    q_ref,
    gain_ref,
    tap_gate,
    tap_value,
    kvx,
    qr,
    ka,
    kb,
    va,
    vb,
    att,
    wo,
    res,
    nrm,
    edge,
    g,
    v,
    d,
    wdown,
    hid,
    part,
    own,
    result,
    rin,
    fin,
    send,
    recv,
    local,
):
    s = lax.axis_index("sp")
    t = lax.axis_index("tp")
    nsp = NZ * NX * NC
    z, x, c = s // (NX * NC), (s // NC) % NX, s % NC

    def at(dz, dx, dc=0):
        return (((z + dz + NZ) % NZ) * NX + (x + dx + NX) % NX) * NC + (c + dc) % NC

    def zi(dz):
        return (z + dz + NZ) % NZ

    def xi(dx):
        return (x + dx + NX) % NX

    ahead, behind = (s + 1) % nsp, (s + nsp - 1) % nsp
    mate = at(0, 0, 1)
    ty = [(t + k) % NY for k in range(NY)]

    cm = Comm(send, recv, local, nrm)

    def cell(weight, dz, dx=0):
        return weight.at[zi(dz), xi(dx), c]

    def grow(dz):
        return g.at[zi(dz), :, c]

    l_v, l_d = cm.here(v_hbm, v.at[z, x, c]), cm.here(d_hbm, d.at[z, x, c])
    l_kv = [
        cm.here(key_hbm, kvx.at[0:HD, pl.ds(WINDOW, ROWS)]),
        cm.here(value_hbm, kvx.at[HD : 2 * HD, pl.ds(WINDOW, ROWS)]),
    ]
    l_wo = cm.here(wo_hbm, wo.at[pl.ds(pl.multiple_of(t * QC, QC), QC)])
    l_g = cm.here(g_hbm, g.at[z, x, c])
    l_q = cm.here(q_hbm, q_ref)
    l_small = [cm.here(gain_hbm, gain_ref), cm.here(tap_gate_hbm, tap_gate), cm.here(tap_value_hbm, tap_value)]
    l_res = cm.here(res_hbm, res)

    barrier = pltpu.get_barrier_semaphore()
    peers = [{"sp": i} for i in (ahead, behind, at(1, 0), at(-1, 0), at(0, 1), at(0, 2), at(0, 3), mate)]
    peers += [{"tp": ty[k]} for k in (1, 3)]
    for peer in peers:
        pl.semaphore_signal(barrier, inc=1, device_id=peer, device_id_type=MESH)
    row = lax.broadcasted_iota(jnp.int32, (WINDOW + 16, 128), 0)
    place = jnp.where(row < WINDOW, row, s * ROWS + (row - WINDOW - 1) * WINDOW).astype(F32)
    angle = place * inverse_ref[...]
    cos_ref[...] = jnp.cos(angle)
    sin_ref[...] = jnp.sin(angle)
    pl.semaphore_wait(barrier, len(peers))

    l_v.wait()

    class Flow:
        def __init__(self, weight, group):
            self.weight, self.group = weight, group
            self.ring, self.across, self.on = {}, {}, {}
            self.push = cm.slot()

        def start(self, ref, slot, **where):
            return cm.start(ref, ref, slot, self.group, **where)

        def begin(self):
            own, self.ring[0] = cell(self.weight, 0), cm.slot()
            self.start(own, self.ring[0], sp=at(1, 0))
            self.start(own, self.ring[0], sp=at(-1, 0))

        def share(self, o, dx=0):
            self.start(cell(self.weight, o, dx), self.push, sp=mate)

        def spread(self, o):
            one, self.across[o] = cell(self.weight, o), cm.slot()
            self.start(one, self.across[o], sp=at(0, 1))
            self.start(one, self.across[o], sp=at(0, -1))

        def round(self, k):
            self.ring[k - 1].wait_recv()
            if k < 4:
                low, high = cell(self.weight, -k), cell(self.weight, k)
                if k == 3:
                    low = self.weight.at[zi(-k), x, c, pl.ds(0, 16)]
                    high = self.weight.at[zi(k), x, c, pl.ds(16, 16)]
                self.ring[k] = cm.slot()
                self.start(low, self.ring[k], sp=at(1, 0))
                self.start(high, self.ring[k], sp=at(-1, 0))

        def pass_on(self, o):
            self.across[o].wait_recv()
            if abs(o) not in self.on:
                self.on[abs(o)] = cm.slot()
            if o >= 0:
                self.start(cell(self.weight, o, -1), self.on[abs(o)], sp=at(0, 1))
            else:
                self.start(cell(self.weight, o, 1), self.on[abs(o)], sp=at(0, -1))
            self.share(o, -1)
            self.share(o, 1)

        def last(self, o):
            self.on[abs(o)].wait_recv()
            self.share(o, 2)

        def arrived(self):
            self.push.wait_recv()

    fv, fd = Flow(v, "v"), Flow(d, "d")
    fv.begin()
    fv.spread(0)
    for copy in l_kv:
        copy.wait()
    halo = cm.slot()
    h_low = cm.start(kvx.at[:, pl.ds(ROWS, WINDOW)], kvx.at[:, pl.ds(0, WINDOW)], halo, sp=ahead)
    h_high = cm.start(kvx.at[:, pl.ds(WINDOW, WINDOW)], kvx.at[:, pl.ds(WINDOW + ROWS, WINDOW)], halo, sp=behind)
    l_wo.wait()

    def worows(k, at_row=0, count=128):
        return wo.at[pl.ds(pl.multiple_of(((t + k) % NY) * QC + c * 128 + at_row, 64), count)]

    wo_first, wo_on, wo_push = cm.slot(), cm.slot(), cm.slot()
    cm.start(worows(0), worows(0), wo_first, "wo", tp=ty[1])
    cm.start(worows(0), worows(0), wo_first, "wo", tp=ty[3])
    l_g.wait()
    g_x, g_push = cm.slot(), cm.slot()
    for k in (1, 3, 2):
        cm.start(g.at[z, x, c], g.at[z, x, c], g_x, "g", sp=at(0, k))
    fv.share(0)
    l_d.wait()
    fd.spread(0)

    def table(b):
        base = pl.ds(WINDOW + b, 1)
        cb, sb = cos_ref[base, :], sin_ref[base, :]
        cr, sr = cos_ref[0:WINDOW, :], sin_ref[0:WINDOW, :]
        lane = lax.broadcasted_iota(jnp.int32, (WINDOW, 128), 1)
        sine = sb * cr + cb * sr
        return cb * cr - sb * sr, jnp.where((lane & 63) < 32, -sine, sine)

    def prepare(b, with_query):
        cosine, sine = table(b)
        rows = pl.ds(pl.multiple_of(b * WINDOW, WINDOW), WINDOW)
        if with_query:
            qrows = pl.ds(pl.multiple_of(b * WINDOW - WINDOW, WINDOW), WINDOW)
            for p in range(2):
                lanes = slice(p * 128, p * 128 + 128)
                qr[qrows, lanes] = turned(q_ref[qrows, lanes].astype(F32), cosine, sine).astype(BF16)
        both = kvx[:, rows].astype(F32).T
        lane = lax.broadcasted_iota(jnp.int32, both.shape, 1)
        keys = jnp.where(lane < HD, turned(both, cosine, sine), 0.0)
        values = jnp.where(lane < HD, 0.0, both)
        ka[rows, :] = keys.astype(BF16)
        kb[rows, :] = pltpu.roll(keys, HD, 1).astype(BF16)
        va[rows, :] = pltpu.roll(values, HD, 1).astype(BF16)
        vb[rows, :] = values.astype(BF16)

    l_q.wait()

    @pl.loop(1, ROWS // WINDOW + 1)
    def _(b):
        prepare(b, True)

    h_low.wait_recv()
    h_high.wait_recv()

    @pl.loop(0, 2)
    def _(i):
        prepare(i * (ROWS // WINDOW + 1), False)

    def attend(b):
        start = pl.multiple_of(b * WINDOW, WINDOW)
        rows = pl.ds(start, WINDOW)
        band = pl.ds(start, 3 * WINDOW)
        r = lax.broadcasted_iota(jnp.int32, (WINDOW, 3 * WINDOW), 0)
        j = lax.broadcasted_iota(jnp.int32, (WINDOW, 3 * WINDOW), 1)
        first = s * ROWS + start - WINDOW
        valid = (j >= r) & (j <= r + 2 * WINDOW) & (j + first >= 0) & (j + first < nsp * ROWS)
        lane = lax.broadcasted_iota(jnp.int32, (WINDOW, 128), 1)
        vv = jnp.concatenate([va[band, :], vb[band, :]], axis=0)
        for p in range(2):
            qp = qr[rows, p * 128 : p * 128 + 128]
            weights, inverse = [], []
            for i, keys in enumerate((ka, kb)):
                sc = lax.dot_general(qp, keys[band, :], NT, preferred_element_type=F32)
                sc = jnp.where(valid, sc * HD ** (-0.5), -1e30)
                sink = sink_ref[2 * p + i]
                top = jnp.maximum(jnp.max(sc, axis=1, keepdims=True), sink)
                w = jnp.exp(sc - top)
                denom = jnp.sum(w, axis=1, keepdims=True) + jnp.exp(sink - top)
                weights.append(w.astype(BF16))
                inverse.append(1.0 / denom)
            o = jnp.dot(jnp.concatenate(weights, axis=1), vv, preferred_element_type=F32)
            o = o * jnp.where(lane < HD, inverse[0], inverse[1])
            att[rows, pl.ds(pl.multiple_of(t * QC + p * 128, 128), 128)] = o.astype(BF16)

    def attend_chunk(ci):
        @pl.loop(0, 2)
        def _(i):
            attend(ci * 2 + i)

    a_y, a_on = {}, {}

    def send_att(ci):
        piece = att.at[pl.ds(ci * CH, CH), pl.ds(pl.multiple_of(t * QC, QC), QC)]
        a_y[ci] = cm.slot()
        cm.start(piece, piece, a_y[ci], tp=ty[1])
        cm.start(piece, piece, a_y[ci], tp=ty[3])

    def pass_att(ci):
        a_y[ci].wait_recv()
        a_on[ci] = cm.slot()
        piece = att.at[pl.ds(ci * CH, 128), pl.ds(pl.multiple_of(ty[3] * QC, QC), QC)]
        cm.start(piece, piece, a_on[ci], tp=ty[1])
        piece = att.at[pl.ds(ci * CH + 128, 128), pl.ds(pl.multiple_of(ty[1] * QC, QC), QC)]
        cm.start(piece, piece, a_on[ci], tp=ty[3])

    def pass_wo():
        wo_first.wait_recv()
        cm.start(worows(3, 0, 64), worows(3, 0, 64), wo_on, "wo", tp=ty[1])
        cm.start(worows(1, 64, 64), worows(1, 64, 64), wo_on, "wo", tp=ty[3])
        cm.start(worows(3), worows(3), wo_push, "wo", sp=mate)
        cm.start(worows(1), worows(1), wo_push, "wo", sp=mate)

    def last_wo():
        wo_on.wait_recv()
        cm.start(worows(2), worows(2), wo_push, "wo", sp=mate)

    g_ring = {}

    def g_send(ref, slot, where):
        cm.start(ref, ref, slot, "g", sp=where)

    def g_first():
        g_x.wait_recv()
        g_ring[0] = cm.slot()
        g_send(grow(0), g_ring[0], at(1, 0))
        g_send(grow(0), g_ring[0], at(-1, 0))
        g_send(grow(0), g_push, mate)

    def g_round(k):
        g_ring[k - 1].wait_recv()
        if k < 4:
            low, high = grow(-k), grow(k)
            if k == 3:
                low, high = g.at[zi(-k), pl.ds(0, 2), c], g.at[zi(k), pl.ds(2, 2), c]
            g_ring[k] = cm.slot()
            g_send(low, g_ring[k], at(1, 0))
            g_send(high, g_ring[k], at(-1, 0))
            g_send(grow(k), g_push, mate)
        g_send(grow(-k), g_push, mate)

    def middle(ci):
        a_on[ci].wait_recv()
        rows = pl.ds(ci * CH, CH)
        nrows = pl.ds(HALO + ci * CH, CH)
        total = jnp.zeros((CH, 1), F32)
        for n in range(D // 512):
            cols = slice(n * 512, n * 512 + 512)
            mid = res[rows, cols].astype(F32) + jnp.dot(att[rows, :], wo[:, cols], preferred_element_type=F32)
            mid = mid.astype(BF16)
            res[rows, cols] = mid
            wide = mid.astype(F32)
            total = total + jnp.sum(wide * wide, axis=1, keepdims=True)
        scale = lax.rsqrt(total / D + EPS)
        for n in range(D // 512):
            cols = slice(n * 512, n * 512 + 512)
            nrm[nrows, cols] = (res[rows, cols].astype(F32) * scale * gain_ref[:, cols]).astype(BF16)

    def up(tc):
        rows = pl.ds(pl.multiple_of(tc * CH, CH), CH + 2 * HALO)
        for n in range(FL // 512):
            cols = slice(n * 512, n * 512 + 512)

            def convolved(weight, taps_ref):
                u = jnp.dot(nrm[rows, :], weight.reshape(D, 512), preferred_element_type=F32)
                u = u.astype(BF16).astype(F32)
                taps = taps_ref[:, cols].astype(F32)
                return (
                    u[HALO - 1 : HALO - 1 + CH] * taps[0:1]
                    + u[HALO : HALO + CH] * taps[1:2]
                    + u[HALO + 1 : HALO + 1 + CH] * taps[2:3]
                )

            gate = convolved(g[:, :, :, :, cols], tap_gate)
            value = convolved(v[:, :, :, :, cols], tap_value)
            hid[:, cols] = (gate / (1.0 + jnp.exp(-gate)) * value).astype(BF16)

    def turn_down():
        for n in range(NZ):
            wdown[:, n * 256 : n * 256 + 256] = d[n].reshape(256, FL).T

    def down(into, tiles=range(D // 512)):
        for n in tiles:
            cols = slice(n * 512, n * 512 + 512)
            into[:, cols] = jnp.dot(hid[...], wdown[:, cols], preferred_element_type=F32).astype(into.dtype)

    attend_chunk(0)
    fv.round(1)
    for o in (1, -1):
        fv.spread(o)
        fv.share(o)
    fv.pass_on(0)
    fd.begin()
    attend_chunk(3)
    send_att(0)
    fv.round(2)
    g_first()
    for o in (2, -2):
        fv.spread(o)
        fv.share(o)
    attend_chunk(1)
    send_att(3)
    fd.round(1)
    fd.spread(1)
    fd.spread(-1)
    attend_chunk(2)
    fv.pass_on(1)
    fv.pass_on(-1)
    fd.pass_on(0)
    fv.last(0)
    fv.round(3)
    for o in (3, -3):
        fv.spread(o)
        fv.share(o)
    pass_wo()
    send_att(1)
    send_att(2)
    fd.round(2)
    g_round(1)
    fv.round(4)
    fv.spread(-4)
    fv.share(-4)
    fd.spread(2)
    fd.spread(-2)
    fv.pass_on(2)
    fv.pass_on(-2)
    fv.last(1)
    fv.last(-1)
    fd.share(0)
    pass_att(0)
    pass_att(3)
    fd.pass_on(1)
    fd.pass_on(-1)
    fd.round(3)
    fd.spread(3)
    fd.spread(-3)
    last_wo()
    fv.pass_on(3)
    fv.pass_on(-3)
    fv.pass_on(-4)
    pass_att(1)
    g_round(2)
    fd.round(4)
    fd.spread(-4)
    pass_att(2)
    for copy in [l_res] + l_small:
        copy.wait()
    fv.last(2)
    fv.last(-2)
    for o in (1, -1, 2, -2):
        fd.share(o)
    wo_push.wait_recv()
    middle(0)
    fd.pass_on(2)
    fd.pass_on(-2)
    middle(3)
    g_round(3)
    e_both = cm.slot()
    cm.start(nrm.at[pl.ds(HALO, HALO)], edge.at[1], e_both, sp=behind)
    middle(1)
    cm.start(nrm.at[pl.ds(ROWS, HALO)], edge.at[0], e_both, sp=ahead)
    fd.pass_on(3)
    fd.pass_on(-3)
    fd.pass_on(-4)
    for o in (3, -3, -4):
        fv.last(o)
    middle(2)
    g_round(4)
    for o in (0, 1, -1, 2, -2):
        fd.last(o)
    fv.arrived()
    g_push.wait_recv()
    e_both.wait_recv()
    nrm[0:HALO, :] = jnp.where(s > 0, edge[0].astype(F32), 0.0).astype(BF16)
    nrm[HALO + ROWS :, :] = jnp.where(s < nsp - 1, edge[1].astype(F32), 0.0).astype(BF16)
    for o in (3, -3, -4):
        fd.share(o)
        fd.last(o)
    up(ty[2])
    fd.arrived()
    turn_down()
    sides = (slice(0, D // 2), slice(D // 2, D))
    s_both = []
    for i, side in enumerate(sides):
        down(part.at[0], (2 * i, 2 * i + 1))
        s_both.append(cm.slot())
        cm.start(part.at[0, 0:128, side], rin.at[0, :, side], s_both[i], "sum", tp=ty[1])
        cm.start(part.at[0, 128:256, side], rin.at[1, :, side], s_both[i], "sum", tp=ty[3])
    up(ty[1])
    down(part.at[1])
    direct = cm.slot()
    cm.start(part.at[1, 128:256], fin.at[1], direct, "sum", tp=ty[1])
    up(ty[3])
    down(part.at[2])
    cm.start(part.at[2, 0:128], fin.at[2], direct, "sum", tp=ty[3])

    def joined(which, rows, side):
        base = 0 if side.start == 0 else D // 2

        @pl.loop(0, 4)
        def _(n):
            cols = pl.ds(pl.multiple_of(base + n * 256, 256), 256)
            total = part[1 + which, rows, cols].astype(F32) + rin[which, :, cols].astype(F32)
            part[1 + which, rows, cols] = total.astype(BF16)

    f_both = []
    for i, side in enumerate(sides):
        s_both[i].wait_recv()
        f_both.append(cm.slot())
        joined(0, slice(0, 128), side)
        cm.start(part.at[1, 0:128, side], fin.at[0, :, side], f_both[i], "sum", tp=ty[1])
        joined(1, slice(128, 256), side)
        cm.start(part.at[2, 128:256, side], fin.at[3, :, side], f_both[i], "sum", tp=ty[3])
    up(t)
    down(own)
    direct.wait_recv()
    written = []
    for i, side in enumerate(sides):
        f_both[i].wait_recv()

        @pl.loop(4 * i, 4 * i + 4)
        def _(n):
            cols = pl.ds(pl.multiple_of(n * 256, 256), 256)
            for k in range(2):
                rows = slice(k * 128, k * 128 + 128)
                mrows = pl.ds(pl.multiple_of(t * CH + k * 128, 128), 128)
                ffn = own[rows, cols] + fin[k, :, cols].astype(F32) + fin[2 + k, :, cols].astype(F32)
                result[rows, cols] = (res[mrows, cols].astype(F32) + ffn).astype(BF16)

        written.append(cm.here(result.at[:, side], out_hbm.at[:, side]))

    cm.sent()
    for copy in written:
        copy.wait()


def shards(
    residual,
    query,
    key,
    value,
    sink,
    norm_gain,
    w_out,
    w_gate,
    w_value,
    conv_gate,
    conv_value,
    w_down,
):
    pair = (jnp.arange(128, dtype=jnp.int32) % (HD // 2) * 2).astype(F32)
    inverse = 1.0 / THETA ** (pair / HD)
    vmem = pl.BlockSpec(memory_space=pltpu.VMEM)
    hbm = pl.BlockSpec(memory_space=pl.ANY)
    return pl.pallas_call(
        layer,
        out_shape=jax.ShapeDtypeStruct((CH, D), BF16),
        in_specs=[pl.BlockSpec(memory_space=pltpu.SMEM)] + [vmem] + [hbm] * 11,
        out_specs=hbm,
        scratch_shapes=[
            pltpu.VMEM((WINDOW + 16, 128), F32),
            pltpu.VMEM((WINDOW + 16, 128), F32),
            pltpu.VMEM((ROWS, QC), BF16),
            pltpu.VMEM((1, D), F32),
            pltpu.VMEM((3, FL), BF16),
            pltpu.VMEM((3, FL), BF16),
            pltpu.VMEM((2 * HD, ROWS + 2 * WINDOW), BF16),
            pltpu.VMEM((ROWS, QC), BF16),
            pltpu.VMEM((ROWS + 2 * WINDOW, 128), BF16),
            pltpu.VMEM((ROWS + 2 * WINDOW, 128), BF16),
            pltpu.VMEM((ROWS + 2 * WINDOW, 128), BF16),
            pltpu.VMEM((ROWS + 2 * WINDOW, 128), BF16),
            pltpu.VMEM((ROWS, NY * QC), BF16),
            pltpu.VMEM((NY * QC, D), BF16),
            pltpu.VMEM((ROWS, D), BF16),
            pltpu.VMEM((ROWS + 2 * HALO, D), BF16),
            pltpu.VMEM((2, HALO, D), BF16),
            pltpu.VMEM((NZ, NX, NC, 32, FL), BF16),
            pltpu.VMEM((NZ, NX, NC, 32, FL), BF16),
            pltpu.VMEM((NZ, NX, NC, 32, FL), BF16),
            pltpu.VMEM((FL, D), BF16),
            pltpu.VMEM((CH, FL), BF16),
            pltpu.VMEM((3, CH, D), BF16),
            pltpu.VMEM((CH, D), F32),
            pltpu.VMEM((CH, D), BF16),
            pltpu.VMEM((2, 128, D), BF16),
            pltpu.VMEM((4, 128, D), BF16),
            pltpu.SemaphoreType.DMA((NSEND,)),
            pltpu.SemaphoreType.DMA((NRECV,)),
            pltpu.SemaphoreType.DMA((NLOC,)),
        ],
        compiler_params=pltpu.CompilerParams(
            collective_id=0, has_side_effects=True, vmem_limit_bytes=62 * 1024 * 1024
        ),
        name="layer",
    )(
        sink,
        inverse.reshape(1, 128),
        query,
        norm_gain.reshape(1, D),
        conv_gate,
        conv_value,
        key.T,
        value.T,
        residual,
        w_out,
        w_gate,
        w_value,
        w_down.T,
    )


def solution(mesh):
    return jax.shard_map(
        shards,
        mesh=mesh,
        in_specs=(
            P("sp", None),
            P("sp", "tp"),
            P("sp", "tp"),
            P("sp", "tp"),
            P("tp"),
            P(),
            P("tp", None),
            P("sp", "tp"),
            P("sp", "tp"),
            P(None, "tp"),
            P(None, "tp"),
            P("tp", "sp"),
        ),
        out_specs=P(("sp", "tp"), None),
        check_vma=False,
    )
```
